128 devices in a mesh: sp: 32 (over z, y, core), tp: 4 (over x).
Axes of the slice: x: 4, y: 4, z: 4, core: 2. Of those that a mesh axis runs over, the one named last changes fastest.
Arguments:
- tokens: bfloat16 [4096, 1024], P('sp', 'tp'), may hold values from -6 to 6
- norm_gain: float32 [1024], replicated, may hold values from 0.1 to 1.9
- attn_query: bfloat16 [1024, 512], P('sp', 'tp'), may hold values from -0.1875 to 0.1875
- attn_key: bfloat16 [1024, 256], P('sp', 'tp'), may hold values from -0.1875 to 0.1875
- attn_value: bfloat16 [1024, 256], P('sp', 'tp'), may hold values from -0.1875 to 0.1875
- sink_logit: float32 [8], P('tp'), may hold values from 2 to 7
- delta_query: bfloat16 [1024, 512], P('sp', 'tp'), may hold values from -0.1875 to 0.1875
- delta_key: bfloat16 [1024, 512], P('sp', 'tp'), may hold values from -0.1875 to 0.1875
- delta_value: bfloat16 [1024, 512], P('sp', 'tp'), may hold values from -0.1875 to 0.1875
- delta_gate: bfloat16 [1024, 512], P('sp', 'tp'), may hold values from -0.1875 to 0.1875
- beta_weight: bfloat16 [1024, 8, 2], P('sp', 'tp'), may hold values from -0.1875 to 0.1875
- decay_weight: bfloat16 [1024, 8, 2], P('sp', 'tp'), may hold values from -0.1875 to 0.1875
- beta_shift: float32 [2, 8], P(None, 'tp'), may hold values from -5 to -2
- decay_log: float32 [2, 8], P(None, 'tp'), may hold values from -2.5 to 1
- out_gain: float32 [64], replicated, may hold values from 0.1 to 1.9
- attn_out: bfloat16 [512, 1024], P('tp', 'sp'), may hold values from -1.5 to 1.5
- delta_out: bfloat16 [512, 1024], P('tp', 'sp'), may hold values from -0.25 to 0.25
Outputs:
- mixed: bfloat16 [4096, 1024], P(('sp', 'tp'))
The draws below stay inside these ranges and needn't reach their ends.
All inputs are finite; a program needn't handle non-finite values.
Results may differ from the reference program's by a relative error of at most 0.0045.
Values may be sent and summed in bfloat16 or wider, within the bound.
A program may use at most 64 MiB of HBM per device.

```python
import jax
import jax.numpy as jnp
from jax import lax

D = 1024
HEAD_DIM = 64
HEADS = 8
KV_HEADS = 4
DELTA_HEADS = 8
WINDOW = 64
TOK_DEV = 128
TOKENS = 4096
N_SP = 32


def shard_levels(stream_key, dims, split, low, largest):
    level, own = 1.0, jax.random.fold_in(stream_key, 6)
    for position, blocks in split:
        steps = jnp.exp(jax.random.uniform(jax.random.fold_in(own, position), (blocks,), jnp.float32, low / len(split), largest / len(split)))
        level = level * jnp.repeat(steps, dims[position] // blocks).reshape([-1 if axis == position else 1 for axis in range(len(dims))])
    return level


def noise(key, dims, scale, bound, shards=(), kind=jnp.bfloat16):
    entries = scale * jax.random.normal(key, dims, jnp.float32)
    if shards:
        entries = entries * shard_levels(key, dims, shards, -0.22, 0.18)
    return jnp.clip(entries, -bound, bound).astype(kind)


def setup_inputs(seed: int = 0) -> dict:
    key_of = jax.random.split(jax.random.key(seed), 18)
    tokens = noise(key_of[0], (TOKENS, D), 1.0, 6.0, ((0, 32), (1, 4)))
    norm_gain = jnp.clip(1.0 + 0.18 * jax.random.normal(key_of[1], (D,), jnp.float32), 0.1, 1.9)
    attn_query = noise(key_of[2], (D, HEADS * HEAD_DIM), D ** -0.5, 0.1875, ((0, 32), (1, 4)))
    attn_key = noise(key_of[3], (D, KV_HEADS * HEAD_DIM), D ** -0.5, 0.1875, ((0, 32), (1, 4)))
    attn_value = noise(key_of[4], (D, KV_HEADS * HEAD_DIM), D ** -0.5, 0.1875, ((0, 32), (1, 4)))
    sink_logit = jnp.clip(2.0 + 5.0 * jax.random.uniform(key_of[5], (HEADS,), jnp.float32) ** shard_levels(key_of[5], (HEADS,), ((0, 4),), -0.2, 0.2), 2.0, 7.0)
    delta_query = noise(key_of[6], (D, DELTA_HEADS * HEAD_DIM), D ** -0.5, 0.1875, ((0, 32), (1, 4)))
    delta_key = noise(key_of[7], (D, DELTA_HEADS * HEAD_DIM), D ** -0.5, 0.1875, ((0, 32), (1, 4)))
    delta_value = noise(key_of[8], (D, DELTA_HEADS * HEAD_DIM), D ** -0.5, 0.1875, ((0, 32), (1, 4)))
    delta_gate = noise(key_of[9], (D, DELTA_HEADS * HEAD_DIM), D ** -0.5, 0.1875, ((0, 32), (1, 4)))
    beta_weight = noise(key_of[10], (D, DELTA_HEADS, 2), D ** -0.5, 0.1875, ((0, 32), (1, 4)))
    decay_weight = noise(key_of[11], (D, DELTA_HEADS, 2), D ** -0.5, 0.1875, ((0, 32), (1, 4)))
    beta_shift = jnp.clip(-5.0 + 3.0 * jax.random.uniform(key_of[12], (2, DELTA_HEADS), jnp.float32) ** shard_levels(key_of[12], (2, DELTA_HEADS), ((1, 4),), -0.2, 0.2), -5.0, -2.0)
    decay_log = jnp.clip(-2.5 + 3.5 * jax.random.uniform(key_of[13], (2, DELTA_HEADS), jnp.float32) ** shard_levels(key_of[13], (2, DELTA_HEADS), ((1, 4),), -0.2, 0.2), -2.5, 1.0)
    out_gain = jnp.clip(1.0 + 0.18 * jax.random.normal(key_of[14], (HEAD_DIM,), jnp.float32), 0.1, 1.9)
    attn_out = noise(key_of[15], (HEADS * HEAD_DIM, D), 16 ** -0.5, 1.5, ((0, 4), (1, 32)))
    delta_out = noise(key_of[16], (DELTA_HEADS * HEAD_DIM, D), (DELTA_HEADS * HEAD_DIM) ** -0.5, 0.25, ((0, 4), (1, 32)))
    return {"tokens": tokens, "norm_gain": norm_gain, "attn_query": attn_query, "attn_key": attn_key, "attn_value": attn_value, "sink_logit": sink_logit, "delta_query": delta_query, "delta_key": delta_key, "delta_value": delta_value, "delta_gate": delta_gate, "beta_weight": beta_weight, "decay_weight": decay_weight, "beta_shift": beta_shift, "decay_log": decay_log, "out_gain": out_gain, "attn_out": attn_out, "delta_out": delta_out}


norm_eps = 1e-06

def rounded(values):
    return lax.optimization_barrier(values.astype(jnp.bfloat16))

def unit_rows(values):
    return values * lax.rsqrt(lax.optimization_barrier(jnp.sum(values * values, axis=-1, keepdims=True)) + norm_eps)

def delta_recur(queries, key_rows, value_rows, log_decay, strength):

    def advance(carry_state, inputs):
        q_row, k_row, v_row, g_row, b_row = inputs
        recall = jnp.einsum('hd,hde->he', k_row, carry_state, precision=lax.Precision.HIGHEST)
        beta_col = b_row[:, None, None]
        carry_state = jnp.exp(g_row)[:, None, None] * (carry_state - beta_col * k_row[:, :, None] * recall[:, None, :]) + beta_col * k_row[:, :, None] * v_row[:, None, :]
        output = jnp.einsum('hd,hde->he', q_row, carry_state, precision=lax.Precision.HIGHEST)
        return (carry_state, output)
    start_state = jnp.zeros((queries.shape[1], queries.shape[2], value_rows.shape[2]), jnp.float32)
    _, outputs = lax.scan(advance, start_state, (queries, key_rows, value_rows, log_decay, strength))
    return outputs

def reference(tokens, norm_gain, attn_query, attn_key, attn_value, sink_logit, delta_query, delta_key, delta_value, delta_gate, beta_weight, decay_weight, beta_shift, decay_log, out_gain, attn_out, delta_out):
    total_rows = tokens.shape[0]
    wide_rows = tokens.astype(jnp.float32)
    inverse = lax.rsqrt(lax.optimization_barrier(jnp.mean(wide_rows * wide_rows, axis=-1, keepdims=True)) + norm_eps)
    normed = (wide_rows * inverse * norm_gain).astype(jnp.bfloat16)

    def project(weight):
        return jnp.dot(normed, weight.reshape(weight.shape[0], -1), preferred_element_type=jnp.float32)
    group_size = HEADS // KV_HEADS
    queries = rounded(project(attn_query)).reshape(total_rows, KV_HEADS, group_size, HEAD_DIM)
    key_rows = rounded(project(attn_key)).reshape(total_rows, KV_HEADS, HEAD_DIM)
    value_rows = rounded(project(attn_value)).reshape(total_rows, KV_HEADS, HEAD_DIM)
    key_pad = jnp.pad(key_rows, ((WINDOW, WINDOW), (0, 0), (0, 0)))
    value_pad = jnp.pad(value_rows, ((WINDOW, WINDOW), (0, 0), (0, 0)))
    sink_row = sink_logit.reshape(KV_HEADS, group_size, 1, 1)
    key_span = TOK_DEV + 2 * WINDOW

    def attend(block_index):
        first_row = block_index * TOK_DEV
        q_block = lax.dynamic_slice_in_dim(queries, first_row, TOK_DEV, 0).astype(jnp.float32)
        k_block = lax.dynamic_slice_in_dim(key_pad, first_row, key_span, 0).astype(jnp.float32)
        v_block = lax.dynamic_slice_in_dim(value_pad, first_row, key_span, 0).astype(jnp.float32)
        scores = jnp.einsum('tkgd,jkd->kgtj', q_block, k_block) * HEAD_DIM ** (-0.5)
        q_pos = first_row + jnp.arange(TOK_DEV, dtype=jnp.int32)
        k_pos = first_row - WINDOW + jnp.arange(key_span, dtype=jnp.int32)
        allowed = (jnp.abs(q_pos[:, None] - k_pos[None, :]) <= WINDOW) & (k_pos[None, :] >= 0) & (k_pos[None, :] < total_rows)
        scores = jnp.where(allowed, scores, -jnp.inf)
        row_max = jnp.maximum(lax.optimization_barrier(jnp.max(scores, axis=-1, keepdims=True)), sink_row)
        weights = jnp.exp(scores - row_max)
        weights = weights / (lax.optimization_barrier(jnp.sum(weights, axis=-1, keepdims=True)) + jnp.exp(sink_row - row_max))
        heads_out = jnp.einsum('kgtj,jkd->tkgd', rounded(weights).astype(jnp.float32), v_block)
        return heads_out.reshape(TOK_DEV, HEADS * HEAD_DIM).astype(jnp.bfloat16)
    y_attn = lax.map(attend, jnp.arange(N_SP, dtype=jnp.int32)).reshape(total_rows, HEADS * HEAD_DIM)

    def activate(weight):
        return jax.nn.silu(rounded(project(weight)).astype(jnp.float32)).reshape(total_rows, DELTA_HEADS, HEAD_DIM)
    d_query = unit_rows(activate(delta_query)) * HEAD_DIM ** (-0.5)
    d_key = unit_rows(activate(delta_key))
    d_value = activate(delta_value)
    gate_rows = rounded(project(delta_gate)).astype(jnp.float32).reshape(total_rows, DELTA_HEADS, HEAD_DIM)
    strength = jax.nn.sigmoid(project(beta_weight).reshape(total_rows, DELTA_HEADS, 2) + beta_shift.T)
    log_decay = -jnp.exp(decay_log.T) * jax.nn.softplus(project(decay_weight).reshape(total_rows, DELTA_HEADS, 2)) / total_rows
    forward = delta_recur(d_query, d_key, d_value, log_decay[:, :, 0], strength[:, :, 0])
    backward = jnp.flip(delta_recur(jnp.flip(d_query, 0), jnp.flip(d_key, 0), jnp.flip(d_value, 0), jnp.flip(log_decay[:, :, 1], 0), jnp.flip(strength[:, :, 1], 0)), 0)
    both_ways = forward + backward
    normed_out = both_ways * lax.rsqrt(lax.optimization_barrier(jnp.mean(both_ways * both_ways, axis=-1, keepdims=True)) + norm_eps) * out_gain
    y_delta = (normed_out * jax.nn.silu(gate_rows)).astype(jnp.bfloat16).reshape(total_rows, DELTA_HEADS * HEAD_DIM)
    summed = jnp.dot(y_attn, attn_out, preferred_element_type=jnp.float32) + jnp.dot(y_delta, delta_out, preferred_element_type=jnp.float32)
    return summed.astype(jnp.bfloat16)
```

```python
import functools

import jax
import jax.numpy as jnp
from jax import lax
from jax.experimental import pallas as pl
from jax.experimental.pallas import tpu as pltpu
from jax.sharding import PartitionSpec as P

HEAD_DIM = 64
WINDOW = 64
norm_eps = 1e-06
MESH = pl.DeviceIdType.MESH
F32 = jnp.float32
BF16 = jnp.bfloat16
SUM_DTYPE = jnp.bfloat16


def exact(a, b, dims=((1,), (0,))):
    return lax.dot_general(
        a, b, (dims, ((), ())), precision=lax.Precision.HIGHEST, preferred_element_type=F32
    )


def plain(a, b, dims=((1,), (0,))):
    return lax.dot_general(a, b, (dims, ((), ())), preferred_element_type=F32)


def split(x):
    high = x.astype(BF16)
    return high, (x - high.astype(F32)).astype(BF16)


def close(a, b, dims=((1,), (0,))):
    (ca,), (cb,) = dims
    left = jnp.concatenate([a[0], a[1], a[0]], axis=ca)
    right = jnp.concatenate([b[0], b[0], b[1]], axis=cb)
    return plain(left, right, dims)


def near(a, b, dims=((1,), (0,))):
    a, b = split(a), split(b)
    return plain(a[0], b[0], dims) + (plain(a[1], b[0], dims) + plain(a[0], b[1], dims))


def silu(x):
    return x * jax.nn.sigmoid(x)


def unit_rows(x):
    return x * lax.rsqrt(jnp.sum(x * x, axis=-1, keepdims=True) + norm_eps)


def copy_to(src, dst, send, recv, device):
    return pltpu.make_async_remote_copy(
        src_ref=src,
        dst_ref=dst,
        send_sem=send,
        recv_sem=recv,
        device_id=device,
        device_id_type=MESH,
    )


RING = 4


def layer_kernel(
    n, nt, heads, kvs, dheads,
    tok, gain, aq, ak, av, dq, dk, dv, dz, ao, do, bw, gw, shift, dlog, sink_in, og, out,
    tokbuf, normed, wbuf, obuf, acc, kvbuf, st, stbuf, o_loc, r_mat, joined, part, rsbuf,
    tok_s, tok_r, w_s, w_r, o_s, o_r, kv_s, kv_r, st_s, st_r, rs_s, rs_r,
):
    me, t = lax.axis_index("sp"), lax.axis_index("tp")
    rows, width = tok.shape
    kb = aq.shape[0]
    hd = HEAD_DIM
    aw, kw, dw = heads * hd, kvs * hd, dheads * hd
    nb = 2 * dheads
    core, chip = lax.rem(me, 2), lax.div(me, 2)
    sa, sb = 1 + (RING - 1) * core, RING - (RING - 1) * core
    pa, pb = lax.rem(lax.div(chip, sa), RING), lax.rem(lax.div(chip, sb), RING)
    partner = me + 1 - 2 * core

    def at_pos(da, db):
        return 2 * (lax.rem(pa + da + RING, RING) * sa + lax.rem(pb + db + RING, RING) * sb) + core

    peers = [at_pos(1, 0), at_pos(-1, 0), at_pos(2, 0), at_pos(0, 1), at_pos(0, -1), at_pos(0, 2)]
    peers.append(partner)
    bar = pltpu.get_barrier_semaphore()
    for p in peers:
        pl.semaphore_signal(bar, inc=1, device_id=(p, t), device_id_type=MESH)
    for d in range(1, nt):
        pl.semaphore_signal(bar, inc=1, device_id=(me, lax.rem(t + d, nt)), device_id_type=MESH)

    mine = pl.ds(me * kb, kb)
    at = 0
    for w in (aq, dq, dk, dv, dz):
        wbuf[mine, at : at + w.shape[1]] = w[...]
        at += w.shape[1]
    wbuf[mine, at : at + 2 * kw] = jnp.concatenate([ak[...], av[...]], axis=1)
    at += 2 * kw
    goff = at
    gates = jnp.concatenate([bw[...], gw[...], gw[...]], axis=0).astype(F32)
    gates = jnp.concatenate([gates, jnp.zeros((128 - 3 * nb, kb), F32)], axis=0)
    gates = jnp.concatenate([gates, jnp.zeros((128, 128 - kb), F32)], axis=1)
    wbuf[mine, goff:] = gates.T[:kb].astype(BF16)
    obuf[mine, :aw] = ao[...]
    obuf[mine, aw:] = do[...]
    tokbuf[t] = tok[...]
    pl.semaphore_wait(bar, len(peers) + nt - 1)

    def w_copy(blk, k, device):
        ref = wbuf.at[pl.ds(blk * kb, kb)]
        return copy_to(ref, ref, w_s.at[k], w_r.at[blk], (device, t))

    sent = []

    def send(blk, k, device):
        c = w_copy(blk, k, device)
        c.start()
        sent.append(c)

    def landed(blk):
        w_copy(blk, 0, partner).wait_recv()

    hops = (0, 1, -1, 2)
    send(me, 0, at_pos(1, 0))
    send(me, 1, at_pos(-1, 0))
    send(me, 2, at_pos(2, 0))
    send(me, 3, at_pos(0, 1))
    send(me, 4, at_pos(0, -1))
    tok_copies = [
        copy_to(tok, tokbuf.at[t], tok_s.at[d - 1], tok_r.at[t], (me, lax.rem(t + d, nt)))
        for d in (1, 3, 2)
    ]
    for c in tok_copies:
        c.start()
    send(me, 15, partner)

    def share(blk, i, db):
        send(blk, 15 + i + RING * (db % RING), partner)

    def first(i):
        blk = at_pos(hops[i], 0)
        landed(blk)
        send(blk, 3 + 3 * i, at_pos(0, 1))
        send(blk, 4 + 3 * i, at_pos(0, -1))
        share(blk, i, 0)

    def second(i):
        for db in (1, -1):
            blk = at_pos(hops[i], db)
            landed(blk)
            if (db == -1) == (i in (0, 2)):
                send(blk, 5 + 3 * i, at_pos(0, -db))
            share(blk, i, db)

    def third(i):
        blk = at_pos(hops[i], 2)
        landed(blk)
        share(blk, i, 2)

    first(1)
    first(2)
    second(0)
    first(3)

    for d in range(1, nt):
        j = lax.rem(t + d, nt)
        copy_to(tok, tokbuf.at[j], tok_s.at[d - 1], tok_r.at[j], (me, j)).wait_recv()
    total = jnp.zeros((rows, 1), F32)
    for j in range(nt):
        x = tokbuf[j].astype(F32)
        total += jnp.sum(x * x, axis=-1, keepdims=True)
    inverse = lax.rsqrt(total / (nt * width) + norm_eps)
    for j in range(nt):
        cols = slice(j * width, (j + 1) * width)
        normed[:, cols] = (tokbuf[j].astype(F32) * inverse * gain[:, cols]).astype(BF16)

    second(1)
    second(2)
    third(0)
    second(3)
    third(1)
    third(2)
    third(3)
    for q in range(n // 2):
        landed(2 * q + 1 - core)

    acc[...] = plain(normed[...], wbuf[...])

    kvbuf[WINDOW : WINDOW + rows] = acc[:, aw + 4 * dw : goff].astype(BF16)

    @pl.when(me == 0)
    def _():
        kvbuf[:WINDOW] = jnp.zeros((WINDOW, 2 * kw), BF16)

    @pl.when(me == n - 1)
    def _():
        kvbuf[WINDOW + rows :] = jnp.zeros((WINDOW, 2 * kw), BF16)

    def head_to(p):
        up = copy_to(
            kvbuf.at[pl.ds(rows, WINDOW)], kvbuf.at[pl.ds(0, WINDOW)],
            kv_s.at[0], kv_r.at[0], (me + 1, t),
        )
        down = copy_to(
            kvbuf.at[pl.ds(WINDOW, WINDOW)], kvbuf.at[pl.ds(WINDOW + rows, WINDOW)],
            kv_s.at[1], kv_r.at[1], (me - 1, t),
        )
        return (up, down)[p]

    pl.when(me < n - 1)(lambda: head_to(0).start())
    pl.when(me > 0)(lambda: head_to(1).start())

    def o_copy(d, blk):
        ref = obuf.at[pl.ds(blk * kb, kb)]
        return copy_to(ref, ref, o_s.at[d], o_r.at[blk], (lax.rem(me + d, n), t))

    for d in range(1, n):
        o_copy(d, me).start()

    base = aw
    lane = lax.broadcasted_iota(jnp.int32, (1, 128), 1)
    shift_row = jnp.zeros((1, 128), F32)
    dlog_row = jnp.zeros((1, 128), F32)
    for h in range(dheads):
        for r in range(2):
            c = h * 2 + r
            shift_row = jnp.where(lane == c, shift[r, h], shift_row)
            dlog_row = jnp.where((lane == nb + c) | (lane == 2 * nb + c), dlog[r, h], dlog_row)
    coef = jnp.where((lane >= nb) & (lane < 3 * nb), -jnp.exp(dlog_row) / (rows * n), 0.0)
    tail = acc[:, goff:]
    soft = jnp.maximum(tail, 0.0) + jnp.log1p(jnp.exp(-jnp.abs(tail)))
    g = coef * soft
    ri = lax.broadcasted_iota(jnp.int32, (rows, rows), 0)
    ci = lax.broadcasted_iota(jnp.int32, (rows, rows), 1)
    incl = (ri >= ci, ri <= ci)
    strict = (ri > ci, ri < ci)
    cums = [exact(jnp.where(m, 1.0, 0.0).astype(F32), g) for m in incl]
    columns = jnp.where(
        lane < nb, jax.nn.sigmoid(tail + shift_row), jnp.where(lane < 2 * nb, cums[0], cums[1])
    )
    lines = columns.T

    chains = []
    for h in range(dheads):
        def cols(i):
            lo_c = base + i * dw + h * hd
            return acc[:, lo_c : lo_c + hd].astype(BF16).astype(F32)

        q = unit_rows(silu(cols(0))) * hd ** (-0.5)
        k = unit_rows(silu(cols(1)))
        v = silu(cols(2))
        kk = near(k, k, ((1,), (1,)))
        qk = near(q, k, ((1,), (1,)))
        for r in range(2):
            c = h * 2 + r
            at = (1 + r) * nb + c
            gcol = columns[:, at : at + 1]
            grow = lines[at : at + 1, :]
            beta = columns[:, c : c + 1]
            decay = jnp.where(incl[r], jnp.exp(jnp.minimum(gcol - grow, 0.0)), 0.0)
            a = jnp.where(strict[r], beta * kk * decay, 0.0)
            eg = jnp.exp(gcol)
            last = gcol[rows - 1 : rows, :] if r == 0 else gcol[0:1, :]
            chains.append(
                dict(
                    r=r, h=h, a=a, rhs=jnp.concatenate([beta * v, beta * k * eg], axis=1),
                    pm=qk * decay, qe=q * eg, kd=(k * jnp.exp(last - gcol)).T, last=last,
                )
            )
    size = 1
    while (1 << size) <= rows:
        size += 1
    levels = size - 1
    eye = jnp.where(ri == ci, 1.0, 0.0).astype(F32)
    xor = ri ^ ci
    inv = [eye - jnp.where(xor == 1, ch["a"], 0.0) for ch in chains]
    pairs = [split(ch["a"]) for ch in chains]
    for lv in range(1, levels):
        m = jnp.where((xor >> lv) == 1, 1.0, 0.0).astype(BF16)
        xs = [split(x) for x in inv]
        left = [close(x, (m * a[0], m * a[1])) for x, a in zip(xs, pairs)]
        inv = [x - close(split(y), z) for x, y, z in zip(inv, left, xs)]
    sols = [split(close(split(x), split(ch["rhs"]))) for x, ch in zip(inv, chains)]
    outs = [close(split(ch["kd"]), s) for ch, s in zip(chains, sols)]
    e64 = jnp.where(
        lax.broadcasted_iota(jnp.int32, (hd, hd), 0)
        == lax.broadcasted_iota(jnp.int32, (hd, hd), 1), 1.0, 0.0,
    ).astype(F32)
    for ch, s in zip(chains, outs):
        full = jnp.concatenate([s[:, :hd], jnp.exp(ch["last"]) * e64 - s[:, hd:]], axis=1)
        st[ch["r"], ch["h"]] = full.astype(BF16)
    def state_copy(r, p):
        return copy_to(st.at[r], stbuf.at[me], st_s.at[p], st_r.at[me], (p, t))

    def state_all(act):
        for d in range(n - 1, 0, -1):
            pl.when(me + d < n)(lambda d=d: act(state_copy(0, me + d)))
            pl.when(me - d >= 0)(lambda d=d: act(state_copy(1, me - d)))

    state_all(lambda c: c.start())
    inner = [close(split(ch["pm"]), s) for ch, s in zip(chains, sols)]
    for ch, s in zip(chains, inner):
        o_loc[ch["r"], ch["h"]] = s[:, :hd]
        r_mat[ch["r"], ch["h"]] = ch["qe"] - s[:, hd:]


    pl.when(me > 0)(lambda: head_to(0).wait_recv())
    pl.when(me < n - 1)(lambda: head_to(1).wait_recv())
    span = rows + 2 * WINDOW
    qi = lax.broadcasted_iota(jnp.int32, (rows, span), 0)
    kj = lax.broadcasted_iota(jnp.int32, (rows, span), 1) - WINDOW
    pos = kj + me * rows
    allowed = (jnp.abs(qi - kj) <= WINDOW) & (pos >= 0) & (pos < n * rows)
    for h in range(heads):
        g = h // (heads // kvs)
        q = acc[:, h * hd : (h + 1) * hd].astype(BF16)
        s = plain(q, kvbuf[:, g * hd : (g + 1) * hd], ((1,), (1,))) * hd ** (-0.5)
        s = jnp.where(allowed, s, -jnp.inf)
        sink = sink_in[h]
        m = jnp.maximum(jnp.max(s, axis=-1, keepdims=True), sink)
        e = jnp.exp(s - m)
        p = e / (jnp.sum(e, axis=-1, keepdims=True) + jnp.exp(sink - m))
        o = plain(p.astype(BF16), kvbuf[:, kw + g * hd : kw + (g + 1) * hd])
        joined[:, h * hd : (h + 1) * hd] = o.astype(BF16)

    for i in range(n):

        @pl.when(me != i)
        def _(i=i):
            copy_to(st.at[0], stbuf.at[i], st_s.at[i], st_r.at[i], (me, t)).wait_recv()

    fore = [jnp.zeros((hd, hd), F32)] * dheads
    back = [jnp.zeros((hd, hd), F32)] * dheads

    def enter(i, state, h, ok):
        both = jnp.where(ok, stbuf[i, h].astype(F32), ident)
        move, (high, low) = both[:, hd:].astype(BF16), split(state)
        return plain(move, high) + plain(move, low) + both[:, :hd]

    ident = jnp.concatenate([jnp.zeros((hd, hd), F32), e64], axis=1)
    for i in range(n - 1):
        fore = [enter(i, x, h, i < me) for h, x in enumerate(fore)]
        back = [enter(n - 1 - i, x, h, n - 1 - i > me) for h, x in enumerate(back)]
    for h in range(dheads):
        o = o_loc[0, h] + o_loc[1, h] + near(r_mat[0, h], fore[h]) + near(r_mat[1, h], back[h])
        o = o * lax.rsqrt(jnp.mean(o * o, axis=-1, keepdims=True) + norm_eps) * og[...]
        lo_c = base + 3 * dw + h * hd
        gate = acc[:, lo_c : lo_c + hd].astype(BF16).astype(F32)
        joined[:, aw + h * hd : aw + (h + 1) * hd] = (o * silu(gate)).astype(BF16)

    for d in range(1, n):
        o_copy(d, lax.rem(me + d, n)).wait_recv()
    tr = rows // nt
    y = plain(joined[...], obuf[...], ((1,), (1,)))
    for j in range(nt):
        part[j] = y[j * tr : (j + 1) * tr].astype(SUM_DTYPE)
    rs_copies = [
        copy_to(
            part.at[lax.rem(t + d, nt)], rsbuf.at[d - 1], rs_s.at[d - 1], rs_r.at[d - 1],
            (me, lax.rem(t + d, nt)),
        )
        for d in range(1, nt)
    ]
    for c in rs_copies:
        c.start()
    for c in tok_copies:
        c.wait_send()
    for c in sent:
        c.wait_send()
    for d in range(1, n):
        o_copy(d, me).wait_send()
    pl.when(me < n - 1)(lambda: head_to(0).wait_send())
    pl.when(me > 0)(lambda: head_to(1).wait_send())
    state_all(lambda c: c.wait_send())
    total = part[t].astype(F32)
    for d in range(1, nt):
        rs_copies[d - 1].wait_recv()
        total += rsbuf[d - 1].astype(F32)
    out[...] = total.astype(BF16)
    for c in rs_copies:
        c.wait_send()


def per_device(
    tokens, norm_gain, attn_query, attn_key, attn_value, sink_logit, delta_query, delta_key,
    delta_value, delta_gate, beta_weight, decay_weight, beta_shift, decay_log, out_gain,
    attn_out, delta_out,
):
    n, nt = lax.axis_size("sp"), lax.axis_size("tp")
    rows, width = tokens.shape
    kb = attn_query.shape[0]
    hd = HEAD_DIM
    heads, kvs = attn_query.shape[1] // hd, attn_key.shape[1] // hd
    dheads = delta_query.shape[1] // hd
    nb = 2 * dheads
    wide = (2 * kvs + heads + 4 * dheads) * hd + 128
    both = (heads + dheads) * hd
    cw = attn_out.shape[1]
    tr = rows // nt
    kw = kvs * hd
    assert n == 2 * RING * RING and cw == kb
    gates = lambda w: jnp.transpose(w, (1, 2, 0)).reshape(nb, kb)
    dma = pltpu.SemaphoreType.DMA
    vm = pl.BlockSpec(memory_space=pltpu.VMEM)
    sm = pl.BlockSpec(memory_space=pltpu.SMEM)
    return pl.pallas_call(
        functools.partial(layer_kernel, n, nt, heads, kvs, dheads),
        out_shape=jax.ShapeDtypeStruct((tr, n * cw), BF16),
        in_specs=[vm] * 13 + [sm] * 3 + [vm],
        out_specs=vm,
        scratch_shapes=[
            pltpu.VMEM((nt, rows, width), BF16),
            pltpu.VMEM((rows, nt * width), BF16),
            pltpu.VMEM((n * kb, wide), BF16),
            pltpu.VMEM((n * cw, both), BF16),
            pltpu.VMEM((rows, wide), F32),
            pltpu.VMEM((rows + 2 * WINDOW, 2 * kw), BF16),
            pltpu.VMEM((2, dheads, hd, 2 * hd), BF16),
            pltpu.VMEM((n, dheads, hd, 2 * hd), BF16),
            pltpu.VMEM((2, dheads, rows, hd), F32),
            pltpu.VMEM((2, dheads, rows, hd), F32),
            pltpu.VMEM((rows, both), BF16),
            pltpu.VMEM((nt, tr, n * cw), SUM_DTYPE),
            pltpu.VMEM((nt - 1, tr, n * cw), SUM_DTYPE),
            dma((nt - 1,)), dma((nt,)),
            dma((n - 1,)), dma((n,)),
            dma((n,)), dma((n,)),
            dma((2,)), dma((2,)),
            dma((n,)), dma((n,)),
            dma((nt - 1,)), dma((nt - 1,)),
        ],
        compiler_params=pltpu.CompilerParams(
            collective_id=0, has_side_effects=True, vmem_limit_bytes=48 * 1024 * 1024
        ),
    )(
        tokens, norm_gain.reshape(1, nt * width), attn_query, attn_key, attn_value, delta_query,
        delta_key, delta_value, delta_gate, attn_out.T, delta_out.T, gates(beta_weight),
        gates(decay_weight), beta_shift, decay_log, sink_logit, out_gain.reshape(1, hd),
    )


def solution(mesh):
    return jax.shard_map(
        per_device,
        mesh=mesh,
        in_specs=(
            P("sp", "tp"), P(), P("sp", "tp"), P("sp", "tp"), P("sp", "tp"), P("tp"),
            P("sp", "tp"), P("sp", "tp"), P("sp", "tp"), P("sp", "tp"),
            P("sp", "tp", None), P("sp", "tp", None), P(None, "tp"), P(None, "tp"), P(),
            P("tp", "sp"), P("tp", "sp"),
        ),
        out_specs=P(("sp", "tp"), None),
        check_vma=False,
    )
```

```python
import functools

import jax
import jax.numpy as jnp
from jax import lax
from jax.experimental import pallas as pl
from jax.experimental.pallas import tpu as pltpu
from jax.sharding import PartitionSpec as P

HEAD_DIM = 64
WINDOW = 64
norm_eps = 1e-06
MESH = pl.DeviceIdType.MESH
F32 = jnp.float32
BF16 = jnp.bfloat16
SUM_DTYPE = jnp.bfloat16
RING = 4


def exact(a, b, dims=((1,), (0,))):
    return lax.dot_general(
        a, b, (dims, ((), ())), precision=lax.Precision.HIGHEST, preferred_element_type=F32
    )


def plain(a, b, dims=((1,), (0,))):
    return lax.dot_general(a, b, (dims, ((), ())), preferred_element_type=F32)


def split(x):
    high = x.astype(BF16)
    return high, (x - high.astype(F32)).astype(BF16)


def close(a, b, dims=((1,), (0,))):
    (ca,), (cb,) = dims
    left = jnp.concatenate([a[0], a[1], a[0]], axis=ca)
    right = jnp.concatenate([b[0], b[0], b[1]], axis=cb)
    return plain(left, right, dims)


def near(a, b, dims=((1,), (0,))):
    a, b = split(a), split(b)
    return plain(a[0], b[0], dims) + (plain(a[1], b[0], dims) + plain(a[0], b[1], dims))


def silu(x):
    return x * jax.nn.sigmoid(x)


def unit_rows(x):
    return x * lax.rsqrt(jnp.sum(x * x, axis=-1, keepdims=True) + norm_eps)


def copy_to(src, dst, send, recv, device):
    return pltpu.make_async_remote_copy(
        src_ref=src,
        dst_ref=dst,
        send_sem=send,
        recv_sem=recv,
        device_id=device,
        device_id_type=MESH,
    )


class Spread:
    def __init__(self, kb, core, z, y, t, buf, own, send_sem, recv_sem):
        self.kb, self.core, self.z, self.y, self.t = kb, core, z, y, t
        self.buf, self.own, self.send_sem, self.recv_sem = buf, own, send_sem, recv_sem
        self.started = []

    def chip(self, axis, da, db):
        dz, dy = (db, da) if axis == 0 else (da, db)
        return lax.rem(self.z + dz + RING, RING) * RING + lax.rem(self.y + dy + RING, RING)

    def send(self, src, blk, device):
        k = len(self.started)
        dst = self.buf.at[pl.ds(blk * self.kb, self.kb)]
        c = copy_to(src, dst, self.send_sem.at[k], self.recv_sem.at[blk], (device, self.t))
        c.start()
        self.started.append(c)

    def landed(self, blk):
        ref = self.buf.at[pl.ds(blk * self.kb, self.kb)]
        partner = 2 * (self.z * RING + self.y) + 1 - self.core
        copy_to(ref, ref, self.send_sem.at[0], self.recv_sem.at[blk], (partner, self.t)).wait_recv()

    def begin(self):
        me = 2 * self.chip(0, 0, 0) + self.core
        for da in (2, 1, -1):
            for axis in (0, 1):
                to = self.chip(axis, da, 0)
                for c in range(2):
                    self.send(self.own(c), me, 2 * to + c)
        self.send(self.own(1 - self.core), me, me + 1 - 2 * self.core)

    def forward(self):
        for r in (1, -1, 2):
            for axis in (0, 1):
                blk = 2 * self.chip(axis, r, 0) + axis
                self.landed(blk)
                for db in (2, 1, -1):
                    src = self.buf.at[pl.ds(blk * self.kb, self.kb)]
                    self.send(src, blk, 2 * self.chip(axis, 0, db) + self.core)

    def finish(self):
        self.landed(2 * self.chip(0, 0, 0) + 1 - self.core)
        for axis in (0, 1):
            for r in (0, 1, -1, 2):
                for db in (1, -1, 2):
                    self.landed(2 * self.chip(axis, r, db) + axis)

    def drain(self):
        for c in self.started:
            c.wait_send()


def layer_kernel(
    n, nt,
    tok_in, gain_in, aq_in, ak_in, av_in, dq_in, dk_in, dv_in, dz_in, ao_in, do_in, bw_in, gw_in,
    shift_in, dlog_in, sink_src, og_in, out,
    gain, wide_in, slim_in, oin, bw, gw, shift, dlog, sink_in, og, in_sem,
    tokbuf, normed, pack, wbuf, obuf, acc, kvbuf, st, stbuf, o_loc, r_mat, heads, other, part, rsbuf,
    tok_s, tok_r, w_s, w_r, o_s, o_r, kv_s, kv_r, st_s, st_r, h_s, h_r, rs_s, rs_r,
):
    me, t = lax.axis_index("sp"), lax.axis_index("tp")
    rows, width = tok_in.shape
    kb = aq_in.shape[0]
    hd = HEAD_DIM
    chips = n // 2
    core, chip = lax.rem(me, 2), lax.div(me, 2)
    z, y = lax.div(chip, RING), lax.rem(chip, RING)
    partner = me + 1 - 2 * core
    mine = pl.ds(me * kb, kb)

    loads = [
        (bw_in, bw), (gw_in, gw), (ak_in, slim_in.at[0]), (av_in, slim_in.at[1]),
        (aq_in, wide_in.at[0]), (dq_in, wide_in.at[1]), (dk_in, wide_in.at[2]),
        (dv_in, wide_in.at[3]), (dz_in, wide_in.at[4]), (ao_in, oin.at[0]), (do_in, oin.at[1]),
        (tok_in, tokbuf.at[t, core]), (gain_in, gain), (shift_in, shift), (dlog_in, dlog),
        (sink_src, sink_in), (og_in, og),
    ]
    loads = [pltpu.make_async_copy(a, b, in_sem.at[i]) for i, (a, b) in enumerate(loads)]
    for c in loads:
        c.start()

    ws = Spread(kb, core, z, y, t, wbuf, lambda c: pack.at[c], w_s, w_r)
    os = Spread(kb, core, z, y, t, obuf, lambda c: obuf.at[mine], o_s, o_r)
    bar = pltpu.get_barrier_semaphore()
    pl.semaphore_signal(bar, inc=1, device_id=(partner, t), device_id_type=MESH)
    for d in range(1, nt):
        pl.semaphore_signal(bar, inc=1, device_id=(me, lax.rem(t + d, nt)), device_id_type=MESH)
    for da in (2, 1, -1):
        for axis in (0, 1):
            for c in range(2):
                p = 2 * ws.chip(axis, da, 0) + c
                pl.semaphore_signal(bar, inc=1, device_id=(p, t), device_id_type=MESH)

    for c in loads:
        c.wait()
    gates = [bw[...], gw[...]]
    lines = []
    for c in range(2):
        lines += [g[2 * c : 2 * c + 2].astype(F32) for g in gates]
        lines.append(jnp.zeros((hd - 4, kb), F32))
    gates = jnp.concatenate(lines, axis=0)
    gates = jnp.concatenate([gates, jnp.zeros((2 * hd, 2 * hd - kb), F32)], axis=1)
    gates = gates.T[:kb].astype(BF16)
    packed = []
    for c in range(2):
        half = slice(c * hd, (c + 1) * hd)
        packed.append(jnp.concatenate(
            [wide_in[i][:, half] for i in range(5)] + [slim_in[0], slim_in[1], gates[:, half]], axis=1
        ))
        pack[c] = packed[c]
    wbuf[mine] = jnp.where(core == 0, packed[0], packed[1])
    obuf[mine] = jnp.concatenate(
        [oin[0][:, :hd], oin[1][:, :hd], oin[0][:, hd:], oin[1][:, hd:]], axis=1
    )
    pl.semaphore_wait(bar, 12 + nt)

    ws.begin()

    def tok_copy(k, j, c, device):
        ref = tokbuf.at[j, c]
        return copy_to(ref, ref, tok_s.at[k], tok_r.at[j, c], device)

    tok_copies = [
        tok_copy(d - 1, t, core, (me, lax.rem(t + d, nt))) for d in (1, 3, 2)
    ] + [tok_copy(nt - 1, t, core, (partner, t))]
    for c in tok_copies:
        c.start()
    ws.forward()
    for d in range(1, nt):
        j = lax.rem(t + d, nt)
        tok_copy(0, j, core, (partner, t)).wait_recv()
        c = tok_copy(nt - 1 + d, j, core, (partner, t))
        c.start()
        tok_copies.append(c)

    def norm(c):
        place = pl.ds(pl.multiple_of(c * rows, rows), rows)
        total = jnp.zeros((rows, 1), F32)
        for j in range(nt):
            x = tokbuf[j, c].astype(F32)
            total += jnp.sum(x * x, axis=-1, keepdims=True)
        inverse = lax.rsqrt(total / (nt * width) + norm_eps)
        for j in range(nt):
            cols = slice(j * width, (j + 1) * width)
            normed[place, cols] = (tokbuf[j, c].astype(F32) * inverse * gain[:, cols]).astype(BF16)

    norm(core)
    for j in range(nt):
        tok_copy(0, j, 1 - core, (partner, t)).wait_recv()
    norm(1 - core)
    os.begin()
    ws.finish()

    acc[...] = plain(normed[...], wbuf[...])
    both = 2 * rows
    kvbuf[WINDOW : WINDOW + both] = acc[:, 5 * hd : 7 * hd].astype(BF16)

    @pl.when(chip == 0)
    def _():
        kvbuf[:WINDOW] = jnp.zeros((WINDOW, 2 * hd), BF16)

    @pl.when(chip == chips - 1)
    def _():
        kvbuf[WINDOW + both :] = jnp.zeros((WINDOW, 2 * hd), BF16)

    def halo(p):
        up = copy_to(
            kvbuf.at[pl.ds(both, WINDOW)], kvbuf.at[pl.ds(0, WINDOW)],
            kv_s.at[0], kv_r.at[0], (me + 2, t),
        )
        down = copy_to(
            kvbuf.at[pl.ds(WINDOW, WINDOW)], kvbuf.at[pl.ds(WINDOW + both, WINDOW)],
            kv_s.at[1], kv_r.at[1], (me - 2, t),
        )
        return (up, down)[p]

    pl.when(chip < chips - 1)(lambda: halo(0).start())
    pl.when(chip > 0)(lambda: halo(1).start())
    os.forward()

    lane = lax.broadcasted_iota(jnp.int32, (1, 2 * hd), 1)
    shift_row = jnp.where(lane == hd, shift[0, core], shift[1, core])
    dlog_row = jnp.where(lane == hd + 2, dlog[0, core], dlog[1, core])
    coef = jnp.where((lane == hd + 2) | (lane == hd + 3), -jnp.exp(dlog_row) / (rows * n), 0.0)
    ri = lax.broadcasted_iota(jnp.int32, (rows, rows), 0)
    ci = lax.broadcasted_iota(jnp.int32, (rows, rows), 1)
    incl = (ri >= ci, ri <= ci)
    strict = (ri > ci, ri < ci)
    ones = [jnp.where(m, 1.0, 0.0).astype(F32) for m in incl]
    chains = []
    for j in range(2):
        part_rows = slice(j * rows, (j + 1) * rows)
        tail = acc[part_rows, 6 * hd :]
        soft = jnp.maximum(tail, 0.0) + jnp.log1p(jnp.exp(-jnp.abs(tail)))
        g = coef * soft
        cums = [exact(m, g) for m in ones]
        columns = jnp.where(
            lane == hd + 2, cums[0],
            jnp.where(lane == hd + 3, cums[1], jax.nn.sigmoid(tail + shift_row)),
        )
        lines = columns.T

        def cols(i):
            return acc[part_rows, i * hd : (i + 1) * hd].astype(BF16).astype(F32)

        q = unit_rows(silu(cols(1))) * hd ** (-0.5)
        k = unit_rows(silu(cols(2)))
        v = silu(cols(3))
        kk = near(k, k, ((1,), (1,)))
        qk = near(q, k, ((1,), (1,)))
        for r in range(2):
            at = hd + 2 + r
            gcol = columns[:, at : at + 1]
            grow = lines[at : at + 1, :]
            beta = columns[:, hd + r : hd + r + 1]
            decay = jnp.where(incl[r], jnp.exp(jnp.minimum(gcol - grow, 0.0)), 0.0)
            a = jnp.where(strict[r], beta * kk * decay, 0.0)
            eg = jnp.exp(gcol)
            last = gcol[rows - 1 : rows, :] if r == 0 else gcol[0:1, :]
            chains.append(
                dict(
                    r=r, j=j, a=a, rhs=jnp.concatenate([beta * v, beta * k * eg], axis=1),
                    pm=qk * decay, qe=q * eg, kd=(k * jnp.exp(last - gcol)).T, last=last,
                )
            )
    levels = rows.bit_length() - 1
    eye = jnp.where(ri == ci, 1.0, 0.0).astype(F32)
    xor = ri ^ ci
    inv = [eye - jnp.where(xor == 1, ch["a"], 0.0) for ch in chains]
    pairs = [split(ch["a"]) for ch in chains]
    for lv in range(1, levels):
        m = jnp.where((xor >> lv) == 1, 1.0, 0.0).astype(BF16)
        xs = [split(x) for x in inv]
        left = [close(x, (m * a[0], m * a[1])) for x, a in zip(xs, pairs)]
        inv = [x - close(split(y_), z_) for x, y_, z_ in zip(inv, left, xs)]
    sols = [split(close(split(x), split(ch["rhs"]))) for x, ch in zip(inv, chains)]
    outs = [close(split(ch["kd"]), s) for ch, s in zip(chains, sols)]
    e64 = jnp.where(
        lax.broadcasted_iota(jnp.int32, (hd, hd), 0)
        == lax.broadcasted_iota(jnp.int32, (hd, hd), 1), 1.0, 0.0,
    ).astype(F32)
    moves = [
        jnp.concatenate([s[:, :hd], jnp.exp(ch["last"]) * e64 - s[:, hd:]], axis=1)
        for ch, s in zip(chains, outs)
    ]
    none = jnp.zeros((hd, hd), F32)
    for r in range(2):
        early, late = moves[2 * r + r], moves[2 * (1 - r) + r]
        full = close(split(late[:, hd:]), split(early))
        full += jnp.concatenate([late[:, :hd], none], axis=1)
        st[r] = full.astype(BF16)

    def state_copy(r, p):
        return copy_to(st.at[r], stbuf.at[chip], st_s.at[p], st_r.at[chip], (2 * p + core, t))

    def state_all(act):
        for d in range(1, chips):
            pl.when(chip + d < chips)(lambda d=d: act(state_copy(0, chip + d)))
            pl.when(chip - d >= 0)(lambda d=d: act(state_copy(1, chip - d)))

    state_all(lambda c: c.start())
    inner = [close(split(ch["pm"]), s) for ch, s in zip(chains, sols)]
    for ch, s in zip(chains, inner):
        o_loc[ch["j"], ch["r"]] = s[:, :hd]
        r_mat[ch["j"], ch["r"]] = ch["qe"] - s[:, hd:]

    pl.when(chip > 0)(lambda: halo(0).wait_recv())
    pl.when(chip < chips - 1)(lambda: halo(1).wait_recv())
    span = rows + 2 * WINDOW
    qi = lax.broadcasted_iota(jnp.int32, (rows, span), 0)
    kj = lax.broadcasted_iota(jnp.int32, (rows, span), 1) - WINDOW
    sink = sink_in[core]
    for j in range(2):
        pos = kj + (2 * chip + j) * rows
        allowed = (jnp.abs(qi - kj) <= WINDOW) & (pos >= 0) & (pos < n * rows)
        q = acc[j * rows : (j + 1) * rows, :hd].astype(BF16)
        keys = slice(j * rows, j * rows + span)
        s = plain(q, kvbuf[keys, :hd], ((1,), (1,))) * hd ** (-0.5)
        s = jnp.where(allowed, s, -jnp.inf)
        m = jnp.maximum(jnp.max(s, axis=-1, keepdims=True), sink)
        e = jnp.exp(s - m)
        p = e / (jnp.sum(e, axis=-1, keepdims=True) + jnp.exp(sink - m))
        heads[j, :, :hd] = plain(p.astype(BF16), kvbuf[keys, hd:]).astype(BF16)

    ident = jnp.concatenate([none, e64], axis=1).astype(BF16)
    sums, prods = [none, none], [e64, e64]
    for d in range(1, chips):
        for r in range(2):
            there = chip - d if r == 0 else chip + d
            ok = there >= 0 if r == 0 else there < chips

            @pl.when(ok)
            def _(there=there):
                copy_to(st.at[0], stbuf.at[there], st_s.at[0], st_r.at[there], (me, t)).wait_recv()

            move = jnp.where(ok, stbuf[jnp.where(ok, there, chip)], ident)
            high, low = split(prods[r])
            step = plain(jnp.concatenate([high, low], axis=1), jnp.concatenate([move, move], axis=0))
            sums[r] = sums[r] + step[:, :hd]
            prods[r] = step[:, hd:]
    for j in range(2):
        o = o_loc[j, 0] + o_loc[j, 1]
        for r in range(2):
            state = sums[r]
            if j != r:
                prev = moves[2 * (1 - j) + r]
                state = near(prev[:, hd:], state) + prev[:, :hd]
            o += near(r_mat[j, r], state)
        o = o * lax.rsqrt(jnp.mean(o * o, axis=-1, keepdims=True) + norm_eps) * og[...]
        gate = acc[j * rows : (j + 1) * rows, 4 * hd : 5 * hd].astype(BF16).astype(F32)
        heads[j, :, hd:] = (o * silu(gate)).astype(BF16)

    hand = copy_to(heads.at[1 - core], other, h_s, h_r, (partner, t))
    hand.start()
    os.finish()
    tr = rows // nt
    side = lambda c: obuf[:, pl.ds(pl.multiple_of(c * 2 * hd, 2 * hd), 2 * hd)]
    result = plain(heads[core], side(core), ((1,), (1,)))
    hand.wait_recv()
    result += plain(other[...], side(1 - core), ((1,), (1,)))
    for j in range(nt):
        part[j] = result[j * tr : (j + 1) * tr].astype(SUM_DTYPE)
    rs_copies = [
        copy_to(
            part.at[lax.rem(t + d, nt)], rsbuf.at[d - 1], rs_s.at[d - 1], rs_r.at[d - 1],
            (me, lax.rem(t + d, nt)),
        )
        for d in range(1, nt)
    ]
    for c in rs_copies:
        c.start()
    for c in tok_copies:
        c.wait_send()
    ws.drain()
    os.drain()
    pl.when(chip < chips - 1)(lambda: halo(0).wait_send())
    pl.when(chip > 0)(lambda: halo(1).wait_send())
    state_all(lambda c: c.wait_send())
    hand.wait_send()
    total = part[t].astype(F32)
    for d in range(1, nt):
        rs_copies[d - 1].wait_recv()
        total += rsbuf[d - 1].astype(F32)
    out[...] = total.astype(BF16)
    for c in rs_copies:
        c.wait_send()


def per_device(
    tokens, norm_gain, attn_query, attn_key, attn_value, sink_logit, delta_query, delta_key,
    delta_value, delta_gate, beta_weight, decay_weight, beta_shift, decay_log, out_gain,
    attn_out, delta_out,
):
    n, nt = lax.axis_size("sp"), lax.axis_size("tp")
    rows, width = tokens.shape
    kb = attn_query.shape[0]
    hd = HEAD_DIM
    cw = attn_out.shape[1]
    tr = rows // nt
    chips = n // 2
    assert n == 2 * RING * RING and cw == kb and rows == 2 * hd
    assert attn_query.shape[1] == delta_query.shape[1] == 2 * attn_key.shape[1] == 2 * hd
    gates = lambda w: jnp.transpose(w, (1, 2, 0)).reshape(4, kb)
    dma = pltpu.SemaphoreType.DMA
    vm, sm = pltpu.VMEM, pltpu.SMEM
    hbm = pl.BlockSpec(memory_space=pltpu.HBM)
    return pl.pallas_call(
        functools.partial(layer_kernel, n, nt),
        out_shape=jax.ShapeDtypeStruct((tr, n * cw), BF16),
        in_specs=[hbm] * 17,
        out_specs=pl.BlockSpec(memory_space=pltpu.VMEM),
        scratch_shapes=[
            vm((1, nt * width), F32),
            vm((5, kb, 2 * hd), BF16),
            vm((2, kb, hd), BF16),
            vm((2, cw, 2 * hd), BF16),
            vm((4, kb), BF16),
            vm((4, kb), BF16),
            sm((2, 2), F32),
            sm((2, 2), F32),
            sm((2,), F32),
            vm((1, hd), F32),
            dma((17,)),
            vm((nt, 2, rows, width), BF16),
            vm((2 * rows, nt * width), BF16),
            vm((2, kb, 8 * hd), BF16),
            vm((n * kb, 8 * hd), BF16),
            vm((n * cw, 4 * hd), BF16),
            vm((2 * rows, 8 * hd), F32),
            vm((2 * rows + 2 * WINDOW, 2 * hd), BF16),
            vm((2, hd, 2 * hd), BF16),
            vm((chips, hd, 2 * hd), BF16),
            vm((2, 2, rows, hd), F32),
            vm((2, 2, rows, hd), F32),
            vm((2, rows, 2 * hd), BF16),
            vm((rows, 2 * hd), BF16),
            vm((nt, tr, n * cw), SUM_DTYPE),
            vm((nt - 1, tr, n * cw), SUM_DTYPE),
            dma((2 * nt - 1,)), dma((nt, 2)),
            dma((n - 1,)), dma((n,)),
            dma((n - 1,)), dma((n,)),
            dma((2,)), dma((2,)),
            dma((chips,)), dma((chips,)),
            dma, dma,
            dma((nt - 1,)), dma((nt - 1,)),
        ],
        compiler_params=pltpu.CompilerParams(
            collective_id=0, has_side_effects=True, vmem_limit_bytes=67043328
        ),
    )(
        tokens, norm_gain.reshape(1, nt * width), attn_query, attn_key, attn_value, delta_query,
        delta_key, delta_value, delta_gate, attn_out.T, delta_out.T, gates(beta_weight),
        gates(decay_weight), beta_shift, decay_log, sink_logit, out_gain.reshape(1, hd),
    )


def solution(mesh):
    return jax.shard_map(
        per_device,
        mesh=mesh,
        in_specs=(
            P("sp", "tp"), P(), P("sp", "tp"), P("sp", "tp"), P("sp", "tp"), P("tp"),
            P("sp", "tp"), P("sp", "tp"), P("sp", "tp"), P("sp", "tp"),
            P("sp", "tp", None), P("sp", "tp", None), P(None, "tp"), P(None, "tp"), P(),
            P("tp", "sp"), P("tp", "sp"),
        ),
        out_specs=P(("sp", "tp"), None),
        check_vma=False,
    )
```

```python
import functools

import jax
import jax.numpy as jnp
from jax import lax
from jax.experimental import pallas as pl
from jax.experimental.pallas import tpu as pltpu
from jax.sharding import PartitionSpec as P

HEAD_DIM = 64
WINDOW = 64
norm_eps = 1e-06
MESH = pl.DeviceIdType.MESH
F32 = jnp.float32
BF16 = jnp.bfloat16
RING = 4


def exact(a, b, dims=((1,), (0,))):
    return lax.dot_general(
        a, b, (dims, ((), ())), precision=lax.Precision.HIGHEST, preferred_element_type=F32
    )


def plain(a, b, dims=((1,), (0,))):
    return lax.dot_general(a, b, (dims, ((), ())), preferred_element_type=F32)


def split(x):
    high = x.astype(BF16)
    return high, (x - high.astype(F32)).astype(BF16)


def close(a, b, dims=((1,), (0,))):
    (ca,), (cb,) = dims
    left = jnp.concatenate([a[0], a[1], a[0]], axis=ca)
    right = jnp.concatenate([b[0], b[0], b[1]], axis=cb)
    return plain(left, right, dims)


def near(a, b, dims=((1,), (0,))):
    a, b = split(a), split(b)
    return plain(a[0], b[0], dims) + (plain(a[1], b[0], dims) + plain(a[0], b[1], dims))


def silu(x):
    return x * jax.nn.sigmoid(x)


def unit_rows(x):
    return x * lax.rsqrt(jnp.sum(x * x, axis=-1, keepdims=True) + norm_eps)


def copy_to(src, dst, send, recv, device):
    return pltpu.make_async_remote_copy(
        src_ref=src,
        dst_ref=dst,
        send_sem=send,
        recv_sem=recv,
        device_id=device,
        device_id_type=MESH,
    )


class Spread:
    def __init__(self, core, z, y, t, rows, own, send_sem, recv_sem, single=False):
        self.core, self.z, self.y, self.t = core, z, y, t
        self.rows, self.own, self.send_sem, self.recv_sem = rows, own, send_sem, recv_sem
        self.single, self.axes = single, (core,) if single else (0, 1)
        self.partner = 2 * (z * RING + y) + 1 - core
        self.started = []

    def chip(self, axis, da, db):
        dz, dy = db + axis * (da - db), da + axis * (db - da)
        return lax.rem(self.z + dz + RING, RING) * RING + lax.rem(self.y + dy + RING, RING)

    def send(self, src, blk, device):
        k = len(self.started)
        c = copy_to(src, self.rows(blk), self.send_sem.at[k], self.recv_sem.at[blk], (device, self.t))
        c.start()
        self.started.append(c)

    def landed(self, blk):
        ref = self.rows(blk)
        copy_to(ref, ref, self.send_sem.at[0], self.recv_sem.at[blk], (self.partner, self.t)).wait_recv()

    def begin(self):
        me = 2 * self.chip(0, 0, 0) + self.core
        for da in (2, 1, -1):
            for axis in (0, 1):
                to = 2 * self.chip(axis, da, 0)
                if self.single:
                    self.send(self.own(self.core), me, to + self.core)
                else:
                    for c in range(2):
                        self.send(self.own(c), me, to + c)
        if not self.single:
            self.send(self.own(1 - self.core), me, self.partner)

    def forward(self):
        for r in (1, -1, 2):
            for axis in self.axes:
                blk = 2 * self.chip(axis, r, 0) + axis
                self.landed(blk)
                for db in (2, 1, -1):
                    self.send(self.rows(blk), blk, 2 * self.chip(axis, 0, db) + self.core)

    def finish(self):
        for r in (0, 1, -1, 2):
            for axis in self.axes:
                for db in (1, -1, 2):
                    self.landed(2 * self.chip(axis, r, db) + axis)
        if not self.single:
            self.landed(self.partner)

    def drain(self):
        for c in self.started:
            c.wait_send()


def layer_kernel(
    n, nt,
    tok_in, gain_in, aq_in, ak_in, av_in, dq_in, dk_in, dv_in, dz_in, ao_in, do_in, bw_in, gw_in,
    shift_in, dlog_in, sink_src, og_in, out,
    gain, wide_in, slim_in, oin, bw, gw, shift, dlog, sink_in, og, in_sem,
    tokbuf, normed, pack1, pack2, wbuf1, wbuf2, obuf, acc1, acc2, kvbuf, st, stbuf, o_loc, r_mat, heads, gath,
    tok_s, tok_r, w1_s, w1_r, w2_s, w2_r, x_s, x_r, g_s, g_r, o_s, o_r, kv_s, kv_r, st_s, st_r, h_s, h_r,
):
    me, t = lax.axis_index("sp"), lax.axis_index("tp")
    rows, width = tok_in.shape
    kb = aq_in.shape[0]
    hd = HEAD_DIM
    chips = n // 2
    core, chip = lax.rem(me, 2), lax.div(me, 2)
    z, y = lax.div(chip, RING), lax.rem(chip, RING)
    partner = me + 1 - 2 * core
    mine = pl.ds(me * kb, kb)

    loads = [
        (bw_in, bw), (gw_in, gw), (ak_in, slim_in.at[0]), (av_in, slim_in.at[1]),
        (aq_in, wide_in.at[0]), (dq_in, wide_in.at[1]), (dk_in, wide_in.at[2]),
        (dv_in, wide_in.at[3]), (dz_in, wide_in.at[4]), (ao_in, oin.at[0]), (do_in, oin.at[1]),
        (tok_in, tokbuf.at[t, core]), (gain_in, gain), (shift_in, shift), (dlog_in, dlog),
        (sink_src, sink_in), (og_in, og),
    ]
    loads = [pltpu.make_async_copy(a, b, in_sem.at[i]) for i, (a, b) in enumerate(loads)]
    for c in loads:
        c.start()

    feats = lambda i: pl.ds(pl.multiple_of(i * 4 * hd, 4 * hd), 4 * hd)
    rows_of = lambda buf: lambda blk: buf.at[pl.ds(blk * kb, kb)]
    o_rows = lambda blk: obuf.at[lax.div(blk, 2), lax.rem(blk, 2), :, feats(t)]
    w1 = Spread(core, z, y, t, rows_of(wbuf1), lambda c: pack1.at[c], w1_s, w1_r)
    w2 = Spread(core, z, y, t, rows_of(wbuf2), lambda c: pack2.at[c], w2_s, w2_r)
    os = Spread(core, z, y, t, o_rows, lambda c: o_rows(me), o_s, o_r, single=True)
    bar = pltpu.get_barrier_semaphore()
    pl.semaphore_signal(bar, inc=1, device_id=(partner, t), device_id_type=MESH)
    for d in range(1, nt):
        pl.semaphore_signal(bar, inc=1, device_id=(me, lax.rem(t + d, nt)), device_id_type=MESH)
    for da in (2, 1, -1):
        for axis in (0, 1):
            for c in range(2):
                p = 2 * w1.chip(axis, da, 0) + c
                pl.semaphore_signal(bar, inc=1, device_id=(p, t), device_id_type=MESH)

    for c in loads:
        c.wait()
    gates = [bw[...], gw[...]]
    lines = []
    for c in range(2):
        lines += [g[2 * c : 2 * c + 2].astype(F32) for g in gates]
        lines.append(jnp.zeros((hd - 4, kb), F32))
    gates = jnp.concatenate(lines, axis=0)
    gates = jnp.concatenate([gates, jnp.zeros((2 * hd, 2 * hd - kb), F32)], axis=1)
    gates = gates.T[:kb].astype(BF16)
    packs = ([], [])
    for c in range(2):
        half = slice(c * hd, (c + 1) * hd)
        aq, dq, dk, dv, dz = [wide_in[i][:, half] for i in range(5)]
        packs[0].append(jnp.concatenate([dk, dv, dq, gates[:, half]], axis=1))
        packs[1].append(jnp.concatenate([aq, dz, slim_in[0], slim_in[1]], axis=1))
        pack1[c], pack2[c] = packs[0][c], packs[1][c]
    wbuf1[mine] = jnp.where(core == 0, packs[0][0], packs[0][1])
    wbuf2[mine] = jnp.where(core == 0, packs[1][0], packs[1][1])
    obuf[chip, core, :, feats(t)] = jnp.concatenate(
        [oin[0][:, :hd], oin[1][:, :hd], oin[0][:, hd:], oin[1][:, hd:]], axis=1
    )
    pl.semaphore_wait(bar, 12 + nt)

    w1.begin()
    w2.begin()

    def tok_copy(k, j, c, device):
        ref = tokbuf.at[j, c]
        return copy_to(ref, ref, tok_s.at[k], tok_r.at[j, c], device)

    tok_copies = [
        tok_copy(d - 1, t, core, (me, lax.rem(t + d, nt))) for d in (1, 3, 2)
    ] + [tok_copy(nt - 1, t, core, (partner, t))]
    for c in tok_copies:
        c.start()

    os.begin()
    w1.forward()
    w2.forward()
    os.forward()
    for d in range(1, nt):
        j = lax.rem(t + d, nt)
        tok_copy(0, j, core, (partner, t)).wait_recv()
        c = tok_copy(nt - 1 + d, j, core, (partner, t))
        c.start()
        tok_copies.append(c)

    def norm(c):
        place = pl.ds(pl.multiple_of(c * rows, rows), rows)
        total = jnp.zeros((rows, 1), F32)
        for j in range(nt):
            x = tokbuf[j, c].astype(F32)
            total += jnp.sum(x * x, axis=-1, keepdims=True)
        inverse = lax.rsqrt(total / (nt * width) + norm_eps)
        for j in range(nt):
            cols = slice(j * width, (j + 1) * width)
            normed[place, cols] = (tokbuf[j, c].astype(F32) * inverse * gain[:, cols]).astype(BF16)

    norm(core)
    for j in range(nt):
        tok_copy(0, j, 1 - core, (partner, t)).wait_recv()
    norm(1 - core)
    w1.finish()

    acc1[...] = plain(normed[...], wbuf1[...])
    os.finish()

    def x_copy(k, j, device):
        ref = obuf.at[:, core, :, feats(j)]
        return copy_to(ref, ref, x_s.at[k], x_r.at[j], (me, device))

    x_copies = [x_copy(d - 1, t, lax.rem(t + d, nt)) for d in range(1, nt)]
    for c in x_copies:
        c.start()

    def share(j, c):
        ref = obuf.at[:, c, :, feats(j)]
        return copy_to(ref, ref, g_s.at[j], g_r.at[j], (partner, t))

    share(t, core).start()

    lane = lax.broadcasted_iota(jnp.int32, (1, 2 * hd), 1)
    shift_row = jnp.where(lane == hd, shift[0, core], shift[1, core])
    dlog_row = jnp.where(lane == hd + 2, dlog[0, core], dlog[1, core])
    coef = jnp.where((lane == hd + 2) | (lane == hd + 3), -jnp.exp(dlog_row) / (rows * n), 0.0)
    ri = lax.broadcasted_iota(jnp.int32, (rows, rows), 0)
    ci = lax.broadcasted_iota(jnp.int32, (rows, rows), 1)
    incl = (ri >= ci, ri <= ci)
    strict = (ri > ci, ri < ci)
    ones = [jnp.where(m, 1.0, 0.0).astype(F32) for m in incl]
    chains = []
    for j in range(2):
        part_rows = slice(j * rows, (j + 1) * rows)
        tail = acc1[part_rows, 2 * hd :]
        soft = jnp.maximum(tail, 0.0) + jnp.log1p(jnp.exp(-jnp.abs(tail)))
        g = coef * soft
        cums = [exact(m, g) for m in ones]
        columns = jnp.where(
            lane == hd + 2, cums[0],
            jnp.where(lane == hd + 3, cums[1], jax.nn.sigmoid(tail + shift_row)),
        )
        lines = columns.T

        def cols(i):
            return acc1[part_rows, i * hd : (i + 1) * hd].astype(BF16).astype(F32)

        q = unit_rows(silu(cols(2))) * hd ** (-0.5)
        k = unit_rows(silu(cols(0)))
        v = silu(cols(1))
        kk = near(k, k, ((1,), (1,)))
        qk = near(q, k, ((1,), (1,)))
        for r in range(2):
            at = hd + 2 + r
            gcol = columns[:, at : at + 1]
            grow = lines[at : at + 1, :]
            beta = columns[:, hd + r : hd + r + 1]
            decay = jnp.where(incl[r], jnp.exp(jnp.minimum(gcol - grow, 0.0)), 0.0)
            a = jnp.where(strict[r], beta * kk * decay, 0.0)
            eg = jnp.exp(gcol)
            last = gcol[rows - 1 : rows, :] if r == 0 else gcol[0:1, :]
            chains.append(
                dict(
                    r=r, j=j, a=a, rhs=jnp.concatenate([beta * v, beta * k * eg], axis=1),
                    pm=qk * decay, qe=q * eg, kd=(k * jnp.exp(last - gcol)).T, last=last,
                )
            )
    levels = rows.bit_length() - 1
    eye = jnp.where(ri == ci, 1.0, 0.0).astype(F32)
    xor = ri ^ ci
    inv = [eye - jnp.where(xor == 1, ch["a"], 0.0) for ch in chains]
    pairs = [split(ch["a"]) for ch in chains]
    for lv in range(1, levels):
        m = jnp.where((xor >> lv) == 1, 1.0, 0.0).astype(BF16)
        xs = [split(x) for x in inv]
        left = [close(x, (m * a[0], m * a[1])) for x, a in zip(xs, pairs)]
        inv = [x - close(split(y_), z_) for x, y_, z_ in zip(inv, left, xs)]
    sols = [split(close(split(x), split(ch["rhs"]))) for x, ch in zip(inv, chains)]
    outs = [close(split(ch["kd"]), s) for ch, s in zip(chains, sols)]
    e64 = jnp.where(
        lax.broadcasted_iota(jnp.int32, (hd, hd), 0)
        == lax.broadcasted_iota(jnp.int32, (hd, hd), 1), 1.0, 0.0,
    ).astype(F32)
    moves = [
        jnp.concatenate([s[:, :hd], jnp.exp(ch["last"]) * e64 - s[:, hd:]], axis=1)
        for ch, s in zip(chains, outs)
    ]
    none = jnp.zeros((hd, hd), F32)
    for r in range(2):
        early, late = moves[2 * r + r], moves[2 * (1 - r) + r]
        full = close(split(late[:, hd:]), split(early))
        full += jnp.concatenate([late[:, :hd], none], axis=1)
        st[r] = full.astype(BF16)

    def state_copy(r, p):
        return copy_to(st.at[r], stbuf.at[chip], st_s.at[p], st_r.at[chip], (2 * p + core, t))

    def state_all(act):
        for d in range(1, chips):
            pl.when(chip + d < chips)(lambda d=d: act(state_copy(0, chip + d)))
            pl.when(chip - d >= 0)(lambda d=d: act(state_copy(1, chip - d)))

    state_all(lambda c: c.start())
    w2.finish()
    acc2[...] = plain(normed[...], wbuf2[...])
    both = 2 * rows
    kvbuf[WINDOW : WINDOW + both] = acc2[:, 2 * hd :].astype(BF16)

    @pl.when(chip == 0)
    def _():
        kvbuf[:WINDOW] = jnp.zeros((WINDOW, 2 * hd), BF16)

    @pl.when(chip == chips - 1)
    def _():
        kvbuf[WINDOW + both :] = jnp.zeros((WINDOW, 2 * hd), BF16)

    def halo(p):
        up = copy_to(
            kvbuf.at[pl.ds(both, WINDOW)], kvbuf.at[pl.ds(0, WINDOW)],
            kv_s.at[0], kv_r.at[0], (me + 2, t),
        )
        down = copy_to(
            kvbuf.at[pl.ds(WINDOW, WINDOW)], kvbuf.at[pl.ds(WINDOW + both, WINDOW)],
            kv_s.at[1], kv_r.at[1], (me - 2, t),
        )
        return (up, down)[p]

    pl.when(chip < chips - 1)(lambda: halo(0).start())
    pl.when(chip > 0)(lambda: halo(1).start())
    inner = [close(split(ch["pm"]), s) for ch, s in zip(chains, sols)]
    for ch, s in zip(chains, inner):
        o_loc[ch["j"], ch["r"]] = s[:, :hd]
        r_mat[ch["j"], ch["r"]] = ch["qe"] - s[:, hd:]

    pl.when(chip > 0)(lambda: halo(0).wait_recv())
    pl.when(chip < chips - 1)(lambda: halo(1).wait_recv())
    span = rows + 2 * WINDOW
    qi = lax.broadcasted_iota(jnp.int32, (rows, span), 0)
    kj = lax.broadcasted_iota(jnp.int32, (rows, span), 1) - WINDOW
    sink = sink_in[core]
    for j in range(2):
        pos = kj + (2 * chip + j) * rows
        allowed = (jnp.abs(qi - kj) <= WINDOW) & (pos >= 0) & (pos < n * rows)
        q = acc2[j * rows : (j + 1) * rows, :hd].astype(BF16)
        keys = slice(j * rows, j * rows + span)
        s = plain(q, kvbuf[keys, :hd], ((1,), (1,))) * hd ** (-0.5)
        s = jnp.where(allowed, s, -jnp.inf)
        m = jnp.maximum(jnp.max(s, axis=-1, keepdims=True), sink)
        e = jnp.exp(s - m)
        p = e / (jnp.sum(e, axis=-1, keepdims=True) + jnp.exp(sink - m))
        heads[j, :, :hd] = plain(p.astype(BF16), kvbuf[keys, hd:]).astype(BF16)

    ident = jnp.concatenate([none, e64], axis=1).astype(BF16)
    sums, prods = [none, none], [e64, e64]
    for d in range(1, chips):
        for r in range(2):
            there = chip - d if r == 0 else chip + d
            ok = there >= 0 if r == 0 else there < chips

            @pl.when(ok)
            def _(there=there):
                copy_to(st.at[0], stbuf.at[there], st_s.at[0], st_r.at[there], (me, t)).wait_recv()

            move = jnp.where(ok, stbuf[jnp.where(ok, there, chip)], ident)
            high, low = split(prods[r])
            step = plain(jnp.concatenate([high, low], axis=1), jnp.concatenate([move, move], axis=0))
            sums[r] = sums[r] + step[:, :hd]
            prods[r] = step[:, hd:]
    for j in range(2):
        o = o_loc[j, 0] + o_loc[j, 1]
        for r in range(2):
            state = sums[r]
            if j != r:
                prev = moves[2 * (1 - j) + r]
                state = near(prev[:, hd:], state) + prev[:, :hd]
            o += near(r_mat[j, r], state)
        o = o * lax.rsqrt(jnp.mean(o * o, axis=-1, keepdims=True) + norm_eps) * og[...]
        gate = acc2[j * rows : (j + 1) * rows, hd : 2 * hd].astype(BF16).astype(F32)
        heads[j, :, hd:] = (o * silu(gate)).astype(BF16)

    tr = rows // nt
    spot = lambda x: pl.ds(pl.multiple_of(x * tr, tr), tr)
    peers = [(lax.rem(t + d, nt), c) for d in range(1, nt) for c in (core, 1 - core)]
    peers.append((t, 1 - core))

    def hand(k, x, c):
        return copy_to(
            heads.at[c, spot(x)], gath.at[2 * t + core], h_s.at[k], h_r.at[2 * t + core], (2 * chip + c, x)
        )

    hands = [hand(k, x, c) for k, (x, c) in enumerate(peers)]
    for c in hands:
        c.start()
    gath[2 * t + core] = heads[core, spot(t)]
    for c in tok_copies + x_copies:
        c.wait_send()
    w1.drain()
    w2.drain()
    os.drain()
    for d in range(1, nt):
        j = lax.rem(t + d, nt)
        x_copy(0, j, j).wait_recv()
        share(j, core).start()
    for j in range(nt):
        share(j, core).wait_send()
        share(j, 1 - core).wait_recv()
    pl.when(chip < chips - 1)(lambda: halo(0).wait_send())
    pl.when(chip > 0)(lambda: halo(1).wait_send())
    state_all(lambda c: c.wait_send())
    for x, c in peers:
        ref = gath.at[2 * x + c]
        copy_to(ref, ref, h_s.at[0], h_r.at[2 * x + c], (2 * chip + c, x)).wait_recv()
    lhs = jnp.concatenate([gath[i] for i in range(2 * nt)], axis=1)
    out[...] = plain(lhs, obuf[...].reshape(n * kb, -1), ((1,), (1,))).astype(BF16)
    for c in hands:
        c.wait_send()


def per_device(
    tokens, norm_gain, attn_query, attn_key, attn_value, sink_logit, delta_query, delta_key,
    delta_value, delta_gate, beta_weight, decay_weight, beta_shift, decay_log, out_gain,
    attn_out, delta_out,
):
    n, nt = lax.axis_size("sp"), lax.axis_size("tp")
    rows, width = tokens.shape
    kb = attn_query.shape[0]
    hd = HEAD_DIM
    cw = attn_out.shape[1]
    tr = rows // nt
    chips = n // 2
    assert n == 2 * RING * RING and cw == kb and rows == 2 * hd
    assert attn_query.shape[1] == delta_query.shape[1] == 2 * attn_key.shape[1] == 2 * hd
    gates = lambda w: jnp.transpose(w, (1, 2, 0)).reshape(4, kb)
    dma = pltpu.SemaphoreType.DMA
    vm, sm = pltpu.VMEM, pltpu.SMEM
    hbm = pl.BlockSpec(memory_space=pltpu.HBM)
    return pl.pallas_call(
        functools.partial(layer_kernel, n, nt),
        out_shape=jax.ShapeDtypeStruct((tr, n * cw), BF16),
        in_specs=[hbm] * 17,
        out_specs=pl.BlockSpec(memory_space=pltpu.VMEM),
        scratch_shapes=[
            vm((1, nt * width), F32),
            vm((5, kb, 2 * hd), BF16),
            vm((2, kb, hd), BF16),
            vm((2, cw, 2 * hd), BF16),
            vm((4, kb), BF16),
            vm((4, kb), BF16),
            sm((2, 2), F32),
            sm((2, 2), F32),
            sm((2,), F32),
            vm((1, hd), F32),
            dma((17,)),
            vm((nt, 2, rows, width), BF16),
            vm((2 * rows, nt * width), BF16),
            vm((2, kb, 4 * hd), BF16),
            vm((2, kb, 4 * hd), BF16),
            vm((n * kb, 4 * hd), BF16),
            vm((n * kb, 4 * hd), BF16),
            vm((chips, 2, cw, nt * 4 * hd), BF16),
            vm((2 * rows, 4 * hd), F32),
            vm((2 * rows, 4 * hd), F32),
            vm((2 * rows + 2 * WINDOW, 2 * hd), BF16),
            vm((2, hd, 2 * hd), BF16),
            vm((chips, hd, 2 * hd), BF16),
            vm((2, 2, rows, hd), F32),
            vm((2, 2, rows, hd), F32),
            vm((2, rows, 2 * hd), BF16),
            vm((2 * nt, tr, 2 * hd), BF16),
            dma((2 * nt - 1,)), dma((nt, 2)),
            dma((n - 1,)), dma((n,)),
            dma((n - 1,)), dma((n,)),
            dma((nt - 1,)), dma((nt,)),
            dma((nt,)), dma((nt,)),
            dma((n - 1,)), dma((n,)),
            dma((2,)), dma((2,)),
            dma((chips,)), dma((chips,)),
            dma((2 * nt - 1,)), dma((2 * nt,)),
        ],
        compiler_params=pltpu.CompilerParams(
            collective_id=0, has_side_effects=True, vmem_limit_bytes=48*1024*1024
        ),
    )(*[pltpu.with_memory_space_constraint(x, pltpu.HBM) for x in (
        tokens, norm_gain.reshape(1, nt * width), attn_query, attn_key, attn_value, delta_query,
        delta_key, delta_value, delta_gate, attn_out.T, delta_out.T, gates(beta_weight),
        gates(decay_weight), beta_shift, decay_log, sink_logit, out_gain.reshape(1, hd),
    )])


def solution(mesh):
    return jax.shard_map(
        per_device,
        mesh=mesh,
        in_specs=(
            P("sp", "tp"), P(), P("sp", "tp"), P("sp", "tp"), P("sp", "tp"), P("tp"),
            P("sp", "tp"), P("sp", "tp"), P("sp", "tp"), P("sp", "tp"),
            P("sp", "tp", None), P("sp", "tp", None), P(None, "tp"), P(None, "tp"), P(),
            P("tp", "sp"), P("tp", "sp"),
        ),
        out_specs=P(("sp", "tp"), None),
        check_vma=False,
    )
```

```python
import functools

import jax
import jax.numpy as jnp
from jax import lax
from jax.experimental import pallas as pl
from jax.experimental.pallas import tpu as pltpu
from jax.sharding import PartitionSpec as P

HEAD_DIM = 64
WINDOW = 64
norm_eps = 1e-06
MESH = pl.DeviceIdType.MESH
F32 = jnp.float32
BF16 = jnp.bfloat16
RING = 4


def exact(a, b, dims=((1,), (0,))):
    return lax.dot_general(
        a, b, (dims, ((), ())), precision=lax.Precision.HIGHEST, preferred_element_type=F32
    )


def plain(a, b, dims=((1,), (0,))):
    return lax.dot_general(a, b, (dims, ((), ())), preferred_element_type=F32)


def split(x):
    high = x.astype(BF16)
    return high, (x - high.astype(F32)).astype(BF16)


def close(a, b, dims=((1,), (0,))):
    (ca,), (cb,) = dims
    left = jnp.concatenate([a[0], a[1], a[0]], axis=ca)
    right = jnp.concatenate([b[0], b[0], b[1]], axis=cb)
    return plain(left, right, dims)


def near(a, b, dims=((1,), (0,))):
    a, b = split(a), split(b)
    return plain(a[0], b[0], dims) + (plain(a[1], b[0], dims) + plain(a[0], b[1], dims))


def silu(x):
    return x * jax.nn.sigmoid(x)


def unit_rows(x):
    return x * lax.rsqrt(jnp.sum(x * x, axis=-1, keepdims=True) + norm_eps)


def copy_to(src, dst, send, recv, device):
    return pltpu.make_async_remote_copy(
        src_ref=src,
        dst_ref=dst,
        send_sem=send,
        recv_sem=recv,
        device_id=device,
        device_id_type=MESH,
    )


class Spread:
    def __init__(self, core, z, y, t, rows, own, send_sem, recv_sem, single=False):
        self.core, self.z, self.y, self.t = core, z, y, t
        self.rows, self.own, self.send_sem, self.recv_sem = rows, own, send_sem, recv_sem
        self.single, self.axes = single, (core,) if single else (0, 1)
        self.partner = 2 * (z * RING + y) + 1 - core
        self.started = []

    def chip(self, axis, da, db):
        dz, dy = db + axis * (da - db), da + axis * (db - da)
        return lax.rem(self.z + dz + RING, RING) * RING + lax.rem(self.y + dy + RING, RING)

    def send(self, src, blk, device):
        k = len(self.started)
        c = copy_to(src, self.rows(blk), self.send_sem.at[k], self.recv_sem.at[blk], (device, self.t))
        c.start()
        self.started.append(c)

    def landed(self, blk):
        ref = self.rows(blk)
        copy_to(ref, ref, self.send_sem.at[0], self.recv_sem.at[blk], (self.partner, self.t)).wait_recv()

    def begin(self):
        me = 2 * self.chip(0, 0, 0) + self.core
        for da in (2, 1, -1):
            for axis in (0, 1):
                to = 2 * self.chip(axis, da, 0)
                if self.single:
                    self.send(self.own(self.core), me, to + self.core)
                else:
                    for c in range(2):
                        self.send(self.own(c), me, to + c)
        if not self.single:
            self.send(self.own(1 - self.core), me, self.partner)

    def forward(self):
        for r in (1, -1, 2):
            for axis in self.axes:
                blk = 2 * self.chip(axis, r, 0) + axis
                self.landed(blk)
                for db in (2, 1, -1):
                    self.send(self.rows(blk), blk, 2 * self.chip(axis, 0, db) + self.core)

    def finish(self, dbs=(1, -1, 2)):
        for r in (0, 1, -1, 2):
            for axis in self.axes:
                for db in dbs:
                    self.landed(2 * self.chip(axis, r, db) + axis)
        if not self.single:
            self.landed(self.partner)

    def drain(self):
        for c in self.started:
            c.wait_send()


def layer_kernel(
    n, nt,
    tok_in, gain_in, aq_in, ak_in, av_in, dq_in, dk_in, dv_in, dz_in, ao_in, do_in, bw_in, gw_in,
    shift_in, dlog_in, sink_src, og_in, out,
    gain, wide_in, slim_in, oin, bw, gw, shift, dlog, sink_in, og, in_sem,
    tokbuf, normed, pack1, pack2, wbuf1, wbuf2, obuf, acc1, acc2, kvbuf, st, stbuf, o_loc, r_mat, heads, gath,
    tok_s, tok_r, w1_s, w1_r, w2_s, w2_r, x_s, x_r, g_s, g_r, o_s, o_r, kv_s, kv_r, st_s, st_r, h_s, h_r,
):
    me, t = lax.axis_index("sp"), lax.axis_index("tp")
    rows, width = tok_in.shape
    kb = aq_in.shape[0]
    hd = HEAD_DIM
    chips = n // 2
    core, chip = lax.rem(me, 2), lax.div(me, 2)
    z, y = lax.div(chip, RING), lax.rem(chip, RING)
    partner = me + 1 - 2 * core
    mine = pl.ds(me * kb, kb)

    loads = [
        (bw_in, bw), (gw_in, gw), (ak_in, slim_in.at[0]), (av_in, slim_in.at[1]),
        (aq_in, wide_in.at[0]), (dq_in, wide_in.at[1]), (dk_in, wide_in.at[2]),
        (dv_in, wide_in.at[3]), (dz_in, wide_in.at[4]), (ao_in, oin.at[0]), (do_in, oin.at[1]),
        (tok_in, tokbuf.at[t, core]), (gain_in, gain), (shift_in, shift), (dlog_in, dlog),
        (sink_src, sink_in), (og_in, og),
    ]
    loads = [pltpu.make_async_copy(a, b, in_sem.at[i]) for i, (a, b) in enumerate(loads)]
    for c in loads:
        c.start()

    feats = lambda i: pl.ds(pl.multiple_of(i * 4 * hd, 4 * hd), 4 * hd)
    rows_of = lambda buf: lambda blk: buf.at[pl.ds(blk * kb, kb)]
    o_rows = lambda blk: obuf.at[lax.div(blk, 2 * RING), lax.rem(lax.div(blk, 2), RING), lax.rem(blk, 2), :, feats(t)]
    w1 = Spread(core, z, y, t, rows_of(wbuf1), lambda c: pack1.at[c], w1_s, w1_r)
    w2 = Spread(core, z, y, t, rows_of(wbuf2), lambda c: pack2.at[c], w2_s, w2_r)
    os = Spread(core, z, y, t, o_rows, lambda c: o_rows(me), o_s, o_r, single=True)
    bar = pltpu.get_barrier_semaphore()
    pl.semaphore_signal(bar, inc=1, device_id=(partner, t), device_id_type=MESH)
    for d in range(1, nt):
        pl.semaphore_signal(bar, inc=1, device_id=(me, lax.rem(t + d, nt)), device_id_type=MESH)
    for da in (2, 1, -1):
        for axis in (0, 1):
            for c in range(2):
                p = 2 * w1.chip(axis, da, 0) + c
                pl.semaphore_signal(bar, inc=1, device_id=(p, t), device_id_type=MESH)

    for c in loads:
        c.wait()
    gates = [bw[...], gw[...]]
    lines = []
    for c in range(2):
        lines += [g[2 * c : 2 * c + 2].astype(F32) for g in gates]
        lines.append(jnp.zeros((hd - 4, kb), F32))
    gates = jnp.concatenate(lines, axis=0)
    gates = jnp.concatenate([gates, jnp.zeros((2 * hd, 2 * hd - kb), F32)], axis=1)
    gates = gates.T[:kb].astype(BF16)
    packs = ([], [])
    for c in range(2):
        half = slice(c * hd, (c + 1) * hd)
        aq, dq, dk, dv, dz = [wide_in[i][:, half] for i in range(5)]
        packs[0].append(jnp.concatenate([dk, dv, dq, gates[:, half]], axis=1))
        packs[1].append(jnp.concatenate([aq, dz, slim_in[0], slim_in[1]], axis=1))
        pack1[c], pack2[c] = packs[0][c], packs[1][c]
    wbuf1[mine] = jnp.where(core == 0, packs[0][0], packs[0][1])
    wbuf2[mine] = jnp.where(core == 0, packs[1][0], packs[1][1])
    obuf[z, y, core, :, feats(t)] = jnp.concatenate(
        [oin[0][:, :hd], oin[1][:, :hd], oin[0][:, hd:], oin[1][:, hd:]], axis=1
    )
    pl.semaphore_wait(bar, 12 + nt)

    w1.begin()

    def tok_copy(k, j, c, device):
        ref = tokbuf.at[j, c]
        return copy_to(ref, ref, tok_s.at[k], tok_r.at[j, c], device)

    tok_copies = [
        tok_copy(d - 1, t, core, (me, lax.rem(t + d, nt))) for d in (1, 3, 2)
    ] + [tok_copy(nt - 1, t, core, (partner, t))]
    for c in tok_copies:
        c.start()

    os.begin()
    w2.begin()
    w1.forward()
    for d in range(1, nt):
        j = lax.rem(t + d, nt)
        tok_copy(0, j, core, (partner, t)).wait_recv()
        c = tok_copy(nt - 1 + d, j, core, (partner, t))
        c.start()
        tok_copies.append(c)

    def norm(c):
        place = pl.ds(pl.multiple_of(c * rows, rows), rows)
        total = jnp.zeros((rows, 1), F32)
        for j in range(nt):
            x = tokbuf[j, c].astype(F32)
            total += jnp.sum(x * x, axis=-1, keepdims=True)
        inverse = lax.rsqrt(total / (nt * width) + norm_eps)
        for j in range(nt):
            cols = slice(j * width, (j + 1) * width)
            normed[place, cols] = (tokbuf[j, c].astype(F32) * inverse * gain[:, cols]).astype(BF16)

    norm(core)
    for j in range(nt):
        tok_copy(0, j, 1 - core, (partner, t)).wait_recv()
    norm(1 - core)
    w2.forward()
    os.forward()

    def own_class(act):
        for c in range(2):
            pl.when(core == c)(lambda c=c: act(c))

    def band(db, c, cols):
        if c == 0:
            return obuf.at[lax.rem(z + db, RING), :, 0, :, cols]
        return obuf.at[:, lax.rem(y + db, RING), 1, :, cols]

    def x_copy(db, d, c, j):
        ref = band(db, c, feats(j))
        return copy_to(ref, ref, x_s.at[db, d - 1], x_r.at[db, j], (me, lax.rem(t + d, nt)))

    def x_all(db, act):
        for d in range(1, nt):
            own_class(lambda c, d=d: act(x_copy(db, d, c, t)))

    def share(db, c):
        ref = band(db, c, pl.ds(0, nt * 4 * hd))
        return copy_to(ref, ref, g_s.at[db], g_r.at[db], (partner, t))

    def pass_on(db):
        for d in range(1, nt):
            own_class(lambda c, d=d: x_copy(db, d, c, lax.rem(t + d, nt)).wait_recv())
        own_class(lambda c: share(db, c).start())

    x_all(0, lambda c: c.start())
    w1.finish()

    acc1[...] = plain(normed[...], wbuf1[...])
    lane = lax.broadcasted_iota(jnp.int32, (1, 2 * hd), 1)
    shift_row = jnp.where(lane == hd, shift[0, core], shift[1, core])
    dlog_row = jnp.where(lane == hd + 2, dlog[0, core], dlog[1, core])
    coef = jnp.where((lane == hd + 2) | (lane == hd + 3), -jnp.exp(dlog_row) / (rows * n), 0.0)
    ri = lax.broadcasted_iota(jnp.int32, (rows, rows), 0)
    ci = lax.broadcasted_iota(jnp.int32, (rows, rows), 1)
    incl = (ri >= ci, ri <= ci)
    strict = (ri > ci, ri < ci)
    ones = [jnp.where(m, 1.0, 0.0).astype(F32) for m in incl]
    chains = []
    for j in range(2):
        part_rows = slice(j * rows, (j + 1) * rows)
        tail = acc1[part_rows, 2 * hd :]
        soft = jnp.maximum(tail, 0.0) + jnp.log1p(jnp.exp(-jnp.abs(tail)))
        g = coef * soft
        cums = [exact(m, g) for m in ones]
        columns = jnp.where(
            lane == hd + 2, cums[0],
            jnp.where(lane == hd + 3, cums[1], jax.nn.sigmoid(tail + shift_row)),
        )
        lines = columns.T

        def cols(i):
            return acc1[part_rows, i * hd : (i + 1) * hd].astype(BF16).astype(F32)

        q = unit_rows(silu(cols(2))) * hd ** (-0.5)
        k = unit_rows(silu(cols(0)))
        v = silu(cols(1))
        kk = near(k, k, ((1,), (1,)))
        qk = near(q, k, ((1,), (1,)))
        for r in range(2):
            at = hd + 2 + r
            gcol = columns[:, at : at + 1]
            grow = lines[at : at + 1, :]
            beta = columns[:, hd + r : hd + r + 1]
            decay = jnp.where(incl[r], jnp.exp(jnp.minimum(gcol - grow, 0.0)), 0.0)
            a = jnp.where(strict[r], beta * kk * decay, 0.0)
            eg = jnp.exp(gcol)
            last = gcol[rows - 1 : rows, :] if r == 0 else gcol[0:1, :]
            chains.append(
                dict(
                    r=r, j=j, a=a, rhs=jnp.concatenate([beta * v, beta * k * eg], axis=1),
                    pm=qk * decay, qe=q * eg, kd=(k * jnp.exp(last - gcol)).T, last=last,
                )
            )
    levels = rows.bit_length() - 1
    eye = jnp.where(ri == ci, 1.0, 0.0).astype(F32)
    xor = ri ^ ci
    inv = [eye - jnp.where(xor == 1, ch["a"], 0.0) for ch in chains]
    pairs = [split(ch["a"]) for ch in chains]
    for lv in range(1, levels):
        m = jnp.where((xor >> lv) == 1, 1.0, 0.0).astype(BF16)
        xs = [split(x) for x in inv]
        left = [close(x, (m * a[0], m * a[1])) for x, a in zip(xs, pairs)]
        inv = [x - close(split(y_), z_) for x, y_, z_ in zip(inv, left, xs)]
    sols = [split(close(split(x), split(ch["rhs"]))) for x, ch in zip(inv, chains)]
    outs = [close(split(ch["kd"]), s) for ch, s in zip(chains, sols)]
    e64 = jnp.where(
        lax.broadcasted_iota(jnp.int32, (hd, hd), 0)
        == lax.broadcasted_iota(jnp.int32, (hd, hd), 1), 1.0, 0.0,
    ).astype(F32)
    moves = [
        jnp.concatenate([s[:, :hd], jnp.exp(ch["last"]) * e64 - s[:, hd:]], axis=1)
        for ch, s in zip(chains, outs)
    ]
    none = jnp.zeros((hd, hd), F32)
    for r in range(2):
        early, late = moves[2 * r + r], moves[2 * (1 - r) + r]
        full = close(split(late[:, hd:]), split(early))
        full += jnp.concatenate([late[:, :hd], none], axis=1)
        st[r] = full.astype(BF16)

    for db in (1, 3, 2):
        os.finish((db if db < 3 else -1,))
        x_all(db, lambda c: c.start())
    def state_copy(r, p):
        return copy_to(st.at[r], stbuf.at[chip], st_s.at[p], st_r.at[chip], (2 * p + core, t))

    def state_all(act):
        for d in range(1, chips):
            pl.when(chip + d < chips)(lambda d=d: act(state_copy(0, chip + d)))
            pl.when(chip - d >= 0)(lambda d=d: act(state_copy(1, chip - d)))

    state_all(lambda c: c.start())
    w2.finish()
    acc2[...] = plain(normed[...], wbuf2[...])
    both = 2 * rows
    kvbuf[WINDOW : WINDOW + both] = acc2[:, 2 * hd :].astype(BF16)

    @pl.when(chip == 0)
    def _():
        kvbuf[:WINDOW] = jnp.zeros((WINDOW, 2 * hd), BF16)

    @pl.when(chip == chips - 1)
    def _():
        kvbuf[WINDOW + both :] = jnp.zeros((WINDOW, 2 * hd), BF16)

    def halo(p):
        up = copy_to(
            kvbuf.at[pl.ds(both, WINDOW)], kvbuf.at[pl.ds(0, WINDOW)],
            kv_s.at[0], kv_r.at[0], (me + 2, t),
        )
        down = copy_to(
            kvbuf.at[pl.ds(WINDOW, WINDOW)], kvbuf.at[pl.ds(WINDOW + both, WINDOW)],
            kv_s.at[1], kv_r.at[1], (me - 2, t),
        )
        return (up, down)[p]

    pl.when(chip < chips - 1)(lambda: halo(0).start())
    pl.when(chip > 0)(lambda: halo(1).start())
    inner = [close(split(ch["pm"]), s) for ch, s in zip(chains, sols)]
    for ch, s in zip(chains, inner):
        o_loc[ch["j"], ch["r"]] = s[:, :hd]
        r_mat[ch["j"], ch["r"]] = ch["qe"] - s[:, hd:]

    pass_on(0)
    pl.when(chip > 0)(lambda: halo(0).wait_recv())
    pl.when(chip < chips - 1)(lambda: halo(1).wait_recv())
    span = rows + 2 * WINDOW
    qi = lax.broadcasted_iota(jnp.int32, (rows, span), 0)
    kj = lax.broadcasted_iota(jnp.int32, (rows, span), 1) - WINDOW
    sink = sink_in[core]
    for j in range(2):
        pos = kj + (2 * chip + j) * rows
        allowed = (jnp.abs(qi - kj) <= WINDOW) & (pos >= 0) & (pos < n * rows)
        q = acc2[j * rows : (j + 1) * rows, :hd].astype(BF16)
        keys = slice(j * rows, j * rows + span)
        s = plain(q, kvbuf[keys, :hd], ((1,), (1,))) * hd ** (-0.5)
        s = jnp.where(allowed, s, -jnp.inf)
        m = jnp.maximum(jnp.max(s, axis=-1, keepdims=True), sink)
        e = jnp.exp(s - m)
        p = e / (jnp.sum(e, axis=-1, keepdims=True) + jnp.exp(sink - m))
        heads[j, :, :hd] = plain(p.astype(BF16), kvbuf[keys, hd:]).astype(BF16)

    for d in range(1, chips):
        there = lax.rem(chip + d, chips)
        copy_to(st.at[0], stbuf.at[there], st_s.at[0], st_r.at[there], (me, t)).wait_recv()

    def follow(late, early):
        full = close(split(late[:, hd:]), split(early))
        return full + jnp.concatenate([late[:, :hd], none], axis=1)

    def first_follow(late, early):
        full = plain(late[:, hd:], early)
        return full + jnp.concatenate([late[:, :hd].astype(F32), none], axis=1)

    ident = jnp.concatenate([none, e64], axis=1)
    kin = []
    for level in range(4):
        size = 1 << level
        before = lax.rem(lax.div(chip, size), 2) == 1
        base = (lax.div(chip, size) + jnp.where(before, -1, 1)) * size
        group = [stbuf[base + i] for i in range(size)]
        merge = first_follow
        while len(group) > 1:
            group = [
                merge(jnp.where(before, hi, lo), jnp.where(before, lo, hi))
                for lo, hi in zip(group[::2], group[1::2])
            ]
            merge = follow
        kin.append((before, group[0].astype(F32)))
    sums = []
    for r in range(2):
        steps = [jnp.where(ok if r == 0 else ~ok, move, ident) for ok, move in kin]
        near_part = follow(follow(steps[0], steps[1]), steps[2])
        sums.append(near(near_part[:, hd:], steps[3][:, :hd]) + near_part[:, :hd])
    for j in range(2):
        o = o_loc[j, 0] + o_loc[j, 1]
        for r in range(2):
            state = sums[r]
            if j != r:
                prev = moves[2 * (1 - j) + r]
                state = near(prev[:, hd:], state) + prev[:, :hd]
            o += near(r_mat[j, r], state)
        o = o * lax.rsqrt(jnp.mean(o * o, axis=-1, keepdims=True) + norm_eps) * og[...]
        gate = acc2[j * rows : (j + 1) * rows, hd : 2 * hd].astype(BF16).astype(F32)
        heads[j, :, hd:] = (o * silu(gate)).astype(BF16)

    tr = rows // nt
    spot = lambda x: pl.ds(pl.multiple_of(x * tr, tr), tr)
    peers = [(lax.rem(t + d, nt), c) for d in range(1, nt) for c in (core, 1 - core)]
    peers.append((t, 1 - core))

    def hand(k, x, c):
        return copy_to(
            heads.at[c, spot(x)], gath.at[2 * t + core], h_s.at[k], h_r.at[2 * t + core], (2 * chip + c, x)
        )

    hands = [hand(k, x, c) for k, (x, c) in enumerate(peers)]
    for c in hands:
        c.start()
    gath[2 * t + core] = heads[core, spot(t)]
    for c in tok_copies:
        c.wait_send()
    w1.drain()
    w2.drain()
    os.drain()
    for db in (1, 3, 2):
        pass_on(db)
    for db in range(RING):
        x_all(db, lambda c: c.wait_send())
        own_class(lambda c: share(db, c).wait_send())
        own_class(lambda c: share(db, 1 - c).wait_recv())
    pl.when(chip < chips - 1)(lambda: halo(0).wait_send())
    pl.when(chip > 0)(lambda: halo(1).wait_send())
    state_all(lambda c: c.wait_send())
    for x, c in peers:
        ref = gath.at[2 * x + c]
        copy_to(ref, ref, h_s.at[0], h_r.at[2 * x + c], (2 * chip + c, x)).wait_recv()
    lhs = jnp.concatenate([gath[i] for i in range(2 * nt)], axis=1)
    out[...] = plain(lhs, obuf[...].reshape(n * kb, -1), ((1,), (1,))).astype(BF16)
    for c in hands:
        c.wait_send()


def per_device(
    tokens, norm_gain, attn_query, attn_key, attn_value, sink_logit, delta_query, delta_key,
    delta_value, delta_gate, beta_weight, decay_weight, beta_shift, decay_log, out_gain,
    attn_out, delta_out,
):
    n, nt = lax.axis_size("sp"), lax.axis_size("tp")
    rows, width = tokens.shape
    kb = attn_query.shape[0]
    hd = HEAD_DIM
    cw = attn_out.shape[1]
    tr = rows // nt
    chips = n // 2
    assert n == 2 * RING * RING and cw == kb and rows == 2 * hd
    assert attn_query.shape[1] == delta_query.shape[1] == 2 * attn_key.shape[1] == 2 * hd
    gates = lambda w: jnp.transpose(w, (1, 2, 0)).reshape(4, kb)
    dma = pltpu.SemaphoreType.DMA
    vm, sm = pltpu.VMEM, pltpu.SMEM
    hbm = pl.BlockSpec(memory_space=pltpu.HBM)
    return pl.pallas_call(
        functools.partial(layer_kernel, n, nt),
        out_shape=jax.ShapeDtypeStruct((tr, n * cw), BF16),
        in_specs=[hbm] * 17,
        out_specs=pl.BlockSpec(memory_space=pltpu.VMEM),
        scratch_shapes=[
            vm((1, nt * width), F32),
            vm((5, kb, 2 * hd), BF16),
            vm((2, kb, hd), BF16),
            vm((2, cw, 2 * hd), BF16),
            vm((4, kb), BF16),
            vm((4, kb), BF16),
            sm((2, 2), F32),
            sm((2, 2), F32),
            sm((2,), F32),
            vm((1, hd), F32),
            dma((17,)),
            vm((nt, 2, rows, width), BF16),
            vm((2 * rows, nt * width), BF16),
            vm((2, kb, 4 * hd), BF16),
            vm((2, kb, 4 * hd), BF16),
            vm((n * kb, 4 * hd), BF16),
            vm((n * kb, 4 * hd), BF16),
            vm((RING, RING, 2, cw, nt * 4 * hd), BF16),
            vm((2 * rows, 4 * hd), F32),
            vm((2 * rows, 4 * hd), F32),
            vm((2 * rows + 2 * WINDOW, 2 * hd), BF16),
            vm((2, hd, 2 * hd), BF16),
            vm((chips, hd, 2 * hd), BF16),
            vm((2, 2, rows, hd), F32),
            vm((2, 2, rows, hd), F32),
            vm((2, rows, 2 * hd), BF16),
            vm((2 * nt, tr, 2 * hd), BF16),
            dma((2 * nt - 1,)), dma((nt, 2)),
            dma((n - 1,)), dma((n,)),
            dma((n - 1,)), dma((n,)),
            dma((RING, nt - 1)), dma((RING, nt)),
            dma((RING,)), dma((RING,)),
            dma((n - 1,)), dma((n,)),
            dma((2,)), dma((2,)),
            dma((chips,)), dma((chips,)),
            dma((2 * nt - 1,)), dma((2 * nt,)),
        ],
        compiler_params=pltpu.CompilerParams(
            collective_id=0, has_side_effects=True, vmem_limit_bytes=48*1024*1024
        ),
    )(*[pltpu.with_memory_space_constraint(x, pltpu.HBM) for x in (
        tokens, norm_gain.reshape(1, nt * width), attn_query, attn_key, attn_value, delta_query,
        delta_key, delta_value, delta_gate, attn_out.T, delta_out.T, gates(beta_weight),
        gates(decay_weight), beta_shift, decay_log, sink_logit, out_gain.reshape(1, hd),
    )])


def solution(mesh):
    return jax.shard_map(
        per_device,
        mesh=mesh,
        in_specs=(
            P("sp", "tp"), P(), P("sp", "tp"), P("sp", "tp"), P("sp", "tp"), P("tp"),
            P("sp", "tp"), P("sp", "tp"), P("sp", "tp"), P("sp", "tp"),
            P("sp", "tp", None), P("sp", "tp", None), P(None, "tp"), P(None, "tp"), P(),
            P("tp", "sp"), P("tp", "sp"),
        ),
        out_specs=P(("sp", "tp"), None),
        check_vma=False,
    )
```

```python
import functools

import jax
import jax.numpy as jnp
from jax import lax
from jax.experimental import pallas as pl
from jax.experimental.pallas import tpu as pltpu
from jax.sharding import PartitionSpec as P

HEAD_DIM = 64
WINDOW = 64
norm_eps = 1e-06
MESH = pl.DeviceIdType.MESH
F32 = jnp.float32
BF16 = jnp.bfloat16
RING = 4


def exact(a, b, dims=((1,), (0,))):
    return lax.dot_general(
        a, b, (dims, ((), ())), precision=lax.Precision.HIGHEST, preferred_element_type=F32
    )


def plain(a, b, dims=((1,), (0,))):
    return lax.dot_general(a, b, (dims, ((), ())), preferred_element_type=F32)


def split(x):
    high = x.astype(BF16)
    return high, (x - high.astype(F32)).astype(BF16)


def close(a, b, dims=((1,), (0,))):
    (ca,), (cb,) = dims
    left = jnp.concatenate([a[0], a[1], a[0]], axis=ca)
    right = jnp.concatenate([b[0], b[0], b[1]], axis=cb)
    return plain(left, right, dims)


def near(a, b, dims=((1,), (0,))):
    a, b = split(a), split(b)
    return plain(a[0], b[0], dims) + (plain(a[1], b[0], dims) + plain(a[0], b[1], dims))


def silu(x):
    return x * jax.nn.sigmoid(x)


def unit_rows(x):
    return x * lax.rsqrt(jnp.sum(x * x, axis=-1, keepdims=True) + norm_eps)


def copy_to(src, dst, send, recv, device):
    return pltpu.make_async_remote_copy(
        src_ref=src,
        dst_ref=dst,
        send_sem=send,
        recv_sem=recv,
        device_id=device,
        device_id_type=MESH,
    )


class Spread:
    def __init__(self, core, z, y, t, rows, own, send_sem, recv_sem, single=False):
        self.core, self.z, self.y, self.t = core, z, y, t
        self.rows, self.own, self.send_sem, self.recv_sem = rows, own, send_sem, recv_sem
        self.single, self.axes = single, (core,) if single else (0, 1)
        self.partner = 2 * (z * RING + y) + 1 - core
        self.started = []

    def chip(self, axis, da, db):
        dz, dy = db + axis * (da - db), da + axis * (db - da)
        return lax.rem(self.z + dz + RING, RING) * RING + lax.rem(self.y + dy + RING, RING)

    def send(self, src, blk, device):
        k = len(self.started)
        c = copy_to(src, self.rows(blk), self.send_sem.at[k], self.recv_sem.at[blk], (device, self.t))
        c.start()
        self.started.append(c)

    def landed(self, blk):
        ref = self.rows(blk)
        copy_to(ref, ref, self.send_sem.at[0], self.recv_sem.at[blk], (self.partner, self.t)).wait_recv()

    def begin(self):
        me = 2 * self.chip(0, 0, 0) + self.core
        for da in (2, 1, -1):
            for axis in (0, 1):
                to = 2 * self.chip(axis, da, 0)
                if self.single:
                    self.send(self.own(self.core), me, to + self.core)
                else:
                    for c in range(2):
                        self.send(self.own(c), me, to + c)
        if not self.single:
            self.send(self.own(1 - self.core), me, self.partner)

    def forward(self):
        for r in (1, -1, 2):
            for axis in self.axes:
                blk = 2 * self.chip(axis, r, 0) + axis
                self.landed(blk)
                for db in (2, 1, -1):
                    self.send(self.rows(blk), blk, 2 * self.chip(axis, 0, db) + self.core)

    def finish(self, dbs=(1, -1, 2)):
        for r in (0, 1, -1, 2):
            for axis in self.axes:
                for db in dbs:
                    self.landed(2 * self.chip(axis, r, db) + axis)
        if not self.single:
            self.landed(self.partner)

    def drain(self):
        for c in self.started:
            c.wait_send()


def layer_kernel(
    n, nt,
    tok_in, gain_in, aq_in, ak_in, av_in, dq_in, dk_in, dv_in, dz_in, ao_in, do_in, bw_in, gw_in,
    shift_in, dlog_in, sink_src, og_in, out,
    gain, wide_in, slim_in, oin, bw, gw, shift, dlog, sink_in, og, in_sem,
    tokbuf, normed, pack1, pack2, wbuf1, wbuf2, obuf, acc1, acc2, kvbuf, st, stbuf, o_loc, r_mat, heads, gath,
    tok_s, tok_r, w1_s, w1_r, w2_s, w2_r, x_s, x_r, g_s, g_r, o_s, o_r, kv_s, kv_r, st_s, st_r, h_s, h_r,
):
    me, t = lax.axis_index("sp"), lax.axis_index("tp")
    rows, width = tok_in.shape
    kb = aq_in.shape[0]
    hd = HEAD_DIM
    chips = n // 2
    core, chip = lax.rem(me, 2), lax.div(me, 2)
    z, y = lax.div(chip, RING), lax.rem(chip, RING)
    partner = me + 1 - 2 * core
    mine = pl.ds(me * kb, kb)

    loads = [
        (bw_in, bw), (gw_in, gw), (ak_in, slim_in.at[0]), (av_in, slim_in.at[1]),
        (aq_in, wide_in.at[0]), (dq_in, wide_in.at[1]), (dk_in, wide_in.at[2]),
        (dv_in, wide_in.at[3]), (dz_in, wide_in.at[4]), (ao_in, oin.at[0]), (do_in, oin.at[1]),
        (tok_in, tokbuf.at[t, core]), (gain_in, gain), (shift_in, shift), (dlog_in, dlog),
        (sink_src, sink_in), (og_in, og),
    ]
    loads = [pltpu.make_async_copy(a, b, in_sem.at[i]) for i, (a, b) in enumerate(loads)]
    for c in loads:
        c.start()

    rows_of = lambda buf: lambda blk: buf.at[pl.ds(blk * kb, kb)]
    o_rows = lambda blk: obuf.at[t, lax.div(blk, 2 * RING), lax.rem(lax.div(blk, 2), RING), lax.rem(blk, 2)]
    w1 = Spread(core, z, y, t, rows_of(wbuf1), lambda c: pack1.at[c], w1_s, w1_r)
    w2 = Spread(core, z, y, t, rows_of(wbuf2), lambda c: pack2.at[c], w2_s, w2_r)
    os = Spread(core, z, y, t, o_rows, lambda c: o_rows(me), o_s, o_r, single=True)
    bar = pltpu.get_barrier_semaphore()
    pl.semaphore_signal(bar, inc=1, device_id=(partner, t), device_id_type=MESH)
    for d in range(1, nt):
        pl.semaphore_signal(bar, inc=1, device_id=(me, lax.rem(t + d, nt)), device_id_type=MESH)
    for da in (2, 1, -1):
        for axis in (0, 1):
            for c in range(2):
                p = 2 * w1.chip(axis, da, 0) + c
                pl.semaphore_signal(bar, inc=1, device_id=(p, t), device_id_type=MESH)

    for c in loads:
        c.wait()
    gates = [bw[...], gw[...]]
    lines = []
    for c in range(2):
        lines += [g[2 * c : 2 * c + 2].astype(F32) for g in gates]
        lines.append(jnp.zeros((hd - 4, kb), F32))
    gates = jnp.concatenate(lines, axis=0)
    gates = jnp.concatenate([gates, jnp.zeros((2 * hd, 2 * hd - kb), F32)], axis=1)
    gates = gates.T[:kb].astype(BF16)
    packs = ([], [])
    for c in range(2):
        half = slice(c * hd, (c + 1) * hd)
        aq, dq, dk, dv, dz = [wide_in[i][:, half] for i in range(5)]
        packs[0].append(jnp.concatenate([dk, dv, dq, gates[:, half]], axis=1))
        packs[1].append(jnp.concatenate([aq, dz, slim_in[0], slim_in[1]], axis=1))
        pack1[c], pack2[c] = packs[0][c], packs[1][c]
    wbuf1[mine] = jnp.where(core == 0, packs[0][0], packs[0][1])
    wbuf2[mine] = jnp.where(core == 0, packs[1][0], packs[1][1])
    obuf[t, z, y, core] = jnp.concatenate(
        [oin[0][:, :hd], oin[1][:, :hd], oin[0][:, hd:], oin[1][:, hd:]], axis=1
    )
    pl.semaphore_wait(bar, 12 + nt)

    w1.begin()

    def tok_copy(k, j, c, device):
        ref = tokbuf.at[j, c]
        return copy_to(ref, ref, tok_s.at[k], tok_r.at[j, c], device)

    tok_copies = [
        tok_copy(d - 1, t, core, (me, lax.rem(t + d, nt))) for d in (1, 3, 2)
    ] + [tok_copy(nt - 1, t, core, (partner, t))]
    for c in tok_copies:
        c.start()

    os.begin()
    w2.begin()
    w1.forward()
    for d in range(1, nt):
        j = lax.rem(t + d, nt)
        tok_copy(0, j, core, (partner, t)).wait_recv()
        c = tok_copy(nt - 1 + d, j, core, (partner, t))
        c.start()
        tok_copies.append(c)

    def norm(c):
        place = pl.ds(pl.multiple_of(c * rows, rows), rows)
        total = jnp.zeros((rows, 1), F32)
        for j in range(nt):
            x = tokbuf[j, c].astype(F32)
            total += jnp.sum(x * x, axis=-1, keepdims=True)
        inverse = lax.rsqrt(total / (nt * width) + norm_eps)
        for j in range(nt):
            cols = slice(j * width, (j + 1) * width)
            normed[place, cols] = (tokbuf[j, c].astype(F32) * inverse * gain[:, cols]).astype(BF16)

    norm(core)
    for j in range(nt):
        tok_copy(0, j, 1 - core, (partner, t)).wait_recv()
    norm(1 - core)
    os.forward()

    def own_class(act):
        for c in range(2):
            pl.when(core == c)(lambda c=c: act(c))

    def band(db, c, j):
        if c == 0:
            return obuf.at[j, lax.rem(z + db, RING), :, 0]
        return obuf.at[j, :, lax.rem(y + db, RING), 1]

    def x_copy(db, d, c, j):
        ref = band(db, c, j)
        return copy_to(ref, ref, x_s.at[db, d - 1], x_r.at[db, j], (me, lax.rem(t + d, nt)))

    def x_all(db, act):
        for d in range(1, nt):
            own_class(lambda c, d=d: act(x_copy(db, d, c, t)))

    def share(db, c):
        ref = band(db, c, slice(None))
        return copy_to(ref, ref, g_s.at[db], g_r.at[db], (partner, t))

    def pass_on(db):
        for d in range(1, nt):
            own_class(lambda c, d=d: x_copy(db, d, c, lax.rem(t + d, nt)).wait_recv())
        own_class(lambda c: share(db, c).start())

    x_all(0, lambda c: c.start())
    w2.forward()
    w1.finish()

    acc1[...] = plain(normed[...], wbuf1[...])
    lane = lax.broadcasted_iota(jnp.int32, (1, 2 * hd), 1)
    shift_row = jnp.where(lane == hd, shift[0, core], shift[1, core])
    dlog_row = jnp.where(lane == hd + 2, dlog[0, core], dlog[1, core])
    coef = jnp.where((lane == hd + 2) | (lane == hd + 3), -jnp.exp(dlog_row) / (rows * n), 0.0)
    ri = lax.broadcasted_iota(jnp.int32, (rows, rows), 0)
    ci = lax.broadcasted_iota(jnp.int32, (rows, rows), 1)
    incl = (ri >= ci, ri <= ci)
    strict = (ri > ci, ri < ci)
    ones = [jnp.where(m, 1.0, 0.0).astype(F32) for m in incl]
    chains = []
    for j in range(2):
        part_rows = slice(j * rows, (j + 1) * rows)
        tail = acc1[part_rows, 2 * hd :]
        soft = jnp.maximum(tail, 0.0) + jnp.log1p(jnp.exp(-jnp.abs(tail)))
        g = coef * soft
        cums = [exact(m, g) for m in ones]
        columns = jnp.where(
            lane == hd + 2, cums[0],
            jnp.where(lane == hd + 3, cums[1], jax.nn.sigmoid(tail + shift_row)),
        )
        lines = columns.T

        def cols(i):
            return acc1[part_rows, i * hd : (i + 1) * hd].astype(BF16).astype(F32)

        q = unit_rows(silu(cols(2))) * hd ** (-0.5)
        k = unit_rows(silu(cols(0)))
        v = silu(cols(1))
        kk = near(k, k, ((1,), (1,)))
        qk = near(q, k, ((1,), (1,)))
        for r in range(2):
            at = hd + 2 + r
            gcol = columns[:, at : at + 1]
            grow = lines[at : at + 1, :]
            beta = columns[:, hd + r : hd + r + 1]
            decay = jnp.where(incl[r], jnp.exp(jnp.minimum(gcol - grow, 0.0)), 0.0)
            a = jnp.where(strict[r], beta * kk * decay, 0.0)
            eg = jnp.exp(gcol)
            last = gcol[rows - 1 : rows, :] if r == 0 else gcol[0:1, :]
            chains.append(
                dict(
                    r=r, j=j, a=a, rhs=jnp.concatenate([beta * v, beta * k * eg], axis=1),
                    pm=qk * decay, qe=q * eg, kd=(k * jnp.exp(last - gcol)).T, last=last,
                )
            )
    levels = rows.bit_length() - 1
    eye = jnp.where(ri == ci, 1.0, 0.0).astype(F32)
    xor = ri ^ ci
    inv = [eye - jnp.where(xor == 1, ch["a"], 0.0) for ch in chains]
    pairs = [split(ch["a"]) for ch in chains]
    for lv in range(1, levels):
        m = jnp.where((xor >> lv) == 1, 1.0, 0.0).astype(BF16)
        xs = [split(x) for x in inv]
        left = [close(x, (m * a[0], m * a[1])) for x, a in zip(xs, pairs)]
        inv = [x - close(split(y_), z_) for x, y_, z_ in zip(inv, left, xs)]
    for db in (1, 3, 2):
        os.finish((db if db < 3 else -1,))
        x_all(db, lambda c: c.start())
    sols = [split(close(split(x), split(ch["rhs"]))) for x, ch in zip(inv, chains)]
    outs = [close(split(ch["kd"]), s) for ch, s in zip(chains, sols)]
    e64 = jnp.where(
        lax.broadcasted_iota(jnp.int32, (hd, hd), 0)
        == lax.broadcasted_iota(jnp.int32, (hd, hd), 1), 1.0, 0.0,
    ).astype(F32)
    moves = [
        jnp.concatenate([s[:, :hd], jnp.exp(ch["last"]) * e64 - s[:, hd:]], axis=1)
        for ch, s in zip(chains, outs)
    ]
    none = jnp.zeros((hd, hd), F32)
    for r in range(2):
        early, late = moves[2 * r + r], moves[2 * (1 - r) + r]
        full = close(split(late[:, hd:]), split(early))
        full += jnp.concatenate([late[:, :hd], none], axis=1)
        st[r] = full.astype(BF16)

    offsets = sorted(
        [(dz, dy) for dz in (0, 1, -1, 2) for dy in (0, 1, -1, 2) if dz or dy], key=lambda o: -abs(o[0]) - abs(o[1])
    )

    def state_copy(k):
        p = w1.chip(0, offsets[k][1], offsets[k][0])
        return copy_to(
            st.at[jnp.where(p > chip, 0, 1)], stbuf.at[chip], st_s.at[k], st_r.at[chip], (2 * p + core, t)
        )

    states = [state_copy(k) for k in range(chips - 1)]
    for c in states:
        c.start()
    w2.finish()
    acc2[...] = plain(normed[...], wbuf2[...])
    both = 2 * rows
    kvbuf[WINDOW : WINDOW + both] = acc2[:, 2 * hd :].astype(BF16)

    @pl.when(chip == 0)
    def _():
        kvbuf[:WINDOW] = jnp.zeros((WINDOW, 2 * hd), BF16)

    @pl.when(chip == chips - 1)
    def _():
        kvbuf[WINDOW + both :] = jnp.zeros((WINDOW, 2 * hd), BF16)

    def halo(p):
        up = copy_to(
            kvbuf.at[pl.ds(both, WINDOW)], kvbuf.at[pl.ds(0, WINDOW)],
            kv_s.at[0], kv_r.at[0], (me + 2, t),
        )
        down = copy_to(
            kvbuf.at[pl.ds(WINDOW, WINDOW)], kvbuf.at[pl.ds(WINDOW + both, WINDOW)],
            kv_s.at[1], kv_r.at[1], (me - 2, t),
        )
        return (up, down)[p]

    pl.when(chip < chips - 1)(lambda: halo(0).start())
    pl.when(chip > 0)(lambda: halo(1).start())
    inner = [close(split(ch["pm"]), s) for ch, s in zip(chains, sols)]
    for ch, s in zip(chains, inner):
        j, r = ch["j"], ch["r"]
        local, reach = s[:, :hd], ch["qe"] - s[:, hd:]
        if j != r:
            step = close(split(reach), split(moves[2 * (1 - j) + r]))
            local, reach = local + step[:, :hd], step[:, hd:]
        o_loc[j, r] = local
        r_mat[j, r] = reach

    pass_on(0)
    pl.when(chip > 0)(lambda: halo(0).wait_recv())
    pl.when(chip < chips - 1)(lambda: halo(1).wait_recv())
    span = rows + 2 * WINDOW
    qi = lax.broadcasted_iota(jnp.int32, (rows, span), 0)
    kj = lax.broadcasted_iota(jnp.int32, (rows, span), 1) - WINDOW
    sink = sink_in[core]
    for j in range(2):
        pos = kj + (2 * chip + j) * rows
        allowed = (jnp.abs(qi - kj) <= WINDOW) & (pos >= 0) & (pos < n * rows)
        q = acc2[j * rows : (j + 1) * rows, :hd].astype(BF16)
        keys = slice(j * rows, j * rows + span)
        s = plain(q, kvbuf[keys, :hd], ((1,), (1,))) * hd ** (-0.5)
        s = jnp.where(allowed, s, -jnp.inf)
        m = jnp.maximum(jnp.max(s, axis=-1, keepdims=True), sink)
        e = jnp.exp(s - m)
        p = e / (jnp.sum(e, axis=-1, keepdims=True) + jnp.exp(sink - m))
        heads[j, :, :hd] = plain(p.astype(BF16), kvbuf[keys, hd:]).astype(BF16)

    for d in range(1, chips):
        there = lax.rem(chip + d, chips)
        copy_to(st.at[0], stbuf.at[there], st_s.at[0], st_r.at[there], (me, t)).wait_recv()

    def follow(late, early):
        full = close(split(late[:, hd:]), split(early))
        return full + jnp.concatenate([late[:, :hd], none], axis=1)

    def first_follow(late, early):
        full = plain(late[:, hd:], early)
        return full + jnp.concatenate([late[:, :hd].astype(F32), none], axis=1)

    ident = jnp.concatenate([none, e64], axis=1)
    kin = []
    for level in range(4):
        size = 1 << level
        before = lax.rem(lax.div(chip, size), 2) == 1
        base = (lax.div(chip, size) + jnp.where(before, -1, 1)) * size
        group = [stbuf[base + i] for i in range(size)]
        merge = first_follow
        while len(group) > 1:
            group = [
                merge(jnp.where(before, hi, lo), jnp.where(before, lo, hi))
                for lo, hi in zip(group[::2], group[1::2])
            ]
            merge = follow
        kin.append((before, group[0].astype(F32)))
    sums = []
    for r in range(2):
        steps = [jnp.where(ok if r == 0 else ~ok, move, ident) for ok, move in kin]
        near_part = follow(follow(steps[0], steps[1]), steps[2])
        sums.append(near(near_part[:, hd:], steps[3][:, :hd]) + near_part[:, :hd])
    for j in range(2):
        o = o_loc[j, 0] + o_loc[j, 1]
        reach = split(jnp.concatenate([r_mat[j, 0], r_mat[j, 1]], axis=1))
        o += close(reach, split(jnp.concatenate(sums, axis=0)))
        o = o * lax.rsqrt(jnp.mean(o * o, axis=-1, keepdims=True) + norm_eps) * og[...]
        gate = acc2[j * rows : (j + 1) * rows, hd : 2 * hd].astype(BF16).astype(F32)
        heads[j, :, hd:] = (o * silu(gate)).astype(BF16)

    tr = rows // nt
    spot = lambda x: pl.ds(pl.multiple_of(x * tr, tr), tr)
    peers = [(lax.rem(t + d, nt), c) for d in range(1, nt) for c in (core, 1 - core)]
    peers.append((t, 1 - core))

    def hand(k, x, c):
        return copy_to(
            heads.at[c, spot(x)], gath.at[2 * t + core], h_s.at[k], h_r.at[2 * t + core], (2 * chip + c, x)
        )

    hands = [hand(k, x, c) for k, (x, c) in enumerate(peers)]
    for c in hands:
        c.start()
    gath[2 * t + core] = heads[core, spot(t)]
    for c in tok_copies:
        c.wait_send()
    w1.drain()
    w2.drain()
    os.drain()
    for db in (1, 3, 2):
        pass_on(db)
    for db in range(RING):
        x_all(db, lambda c: c.wait_send())
        own_class(lambda c: share(db, c).wait_send())
        own_class(lambda c: share(db, 1 - c).wait_recv())
    pl.when(chip < chips - 1)(lambda: halo(0).wait_send())
    pl.when(chip > 0)(lambda: halo(1).wait_send())
    for c in states:
        c.wait_send()
    for x, c in peers:
        ref = gath.at[2 * x + c]
        copy_to(ref, ref, h_s.at[0], h_r.at[2 * x + c], (2 * chip + c, x)).wait_recv()
    total = jnp.zeros(out.shape, F32)
    for x in range(nt):
        lhs = jnp.concatenate([gath[2 * x], gath[2 * x + 1]], axis=1)
        total += plain(lhs, obuf[x].reshape(n * kb, -1), ((1,), (1,)))
    out[...] = total.astype(BF16)
    for c in hands:
        c.wait_send()


def per_device(
    tokens, norm_gain, attn_query, attn_key, attn_value, sink_logit, delta_query, delta_key,
    delta_value, delta_gate, beta_weight, decay_weight, beta_shift, decay_log, out_gain,
    attn_out, delta_out,
):
    n, nt = lax.axis_size("sp"), lax.axis_size("tp")
    rows, width = tokens.shape
    kb = attn_query.shape[0]
    hd = HEAD_DIM
    cw = attn_out.shape[1]
    tr = rows // nt
    chips = n // 2
    assert n == 2 * RING * RING and cw == kb and rows == 2 * hd
    assert attn_query.shape[1] == delta_query.shape[1] == 2 * attn_key.shape[1] == 2 * hd
    gates = lambda w: jnp.transpose(w, (1, 2, 0)).reshape(4, kb)
    dma = pltpu.SemaphoreType.DMA
    vm, sm = pltpu.VMEM, pltpu.SMEM
    hbm = pl.BlockSpec(memory_space=pltpu.HBM)
    return pl.pallas_call(
        functools.partial(layer_kernel, n, nt),
        out_shape=jax.ShapeDtypeStruct((tr, n * cw), BF16),
        in_specs=[hbm] * 17,
        out_specs=pl.BlockSpec(memory_space=pltpu.VMEM),
        scratch_shapes=[
            vm((1, nt * width), F32),
            vm((5, kb, 2 * hd), BF16),
            vm((2, kb, hd), BF16),
            vm((2, cw, 2 * hd), BF16),
            vm((4, kb), BF16),
            vm((4, kb), BF16),
            sm((2, 2), F32),
            sm((2, 2), F32),
            sm((2,), F32),
            vm((1, hd), F32),
            dma((17,)),
            vm((nt, 2, rows, width), BF16),
            vm((2 * rows, nt * width), BF16),
            vm((2, kb, 4 * hd), BF16),
            vm((2, kb, 4 * hd), BF16),
            vm((n * kb, 4 * hd), BF16),
            vm((n * kb, 4 * hd), BF16),
            vm((nt, RING, RING, 2, cw, 4 * hd), BF16),
            vm((2 * rows, 4 * hd), F32),
            vm((2 * rows, 4 * hd), F32),
            vm((2 * rows + 2 * WINDOW, 2 * hd), BF16),
            vm((2, hd, 2 * hd), BF16),
            vm((chips, hd, 2 * hd), BF16),
            vm((2, 2, rows, hd), F32),
            vm((2, 2, rows, hd), F32),
            vm((2, rows, 2 * hd), BF16),
            vm((2 * nt, tr, 2 * hd), BF16),
            dma((2 * nt - 1,)), dma((nt, 2)),
            dma((n - 1,)), dma((n,)),
            dma((n - 1,)), dma((n,)),
            dma((RING, nt - 1)), dma((RING, nt)),
            dma((RING,)), dma((RING,)),
            dma((n - 1,)), dma((n,)),
            dma((2,)), dma((2,)),
            dma((chips,)), dma((chips,)),
            dma((2 * nt - 1,)), dma((2 * nt,)),
        ],
        compiler_params=pltpu.CompilerParams(
            collective_id=0, has_side_effects=True, vmem_limit_bytes=48*1024*1024
        ),
    )(*[pltpu.with_memory_space_constraint(x, pltpu.HBM) for x in (
        tokens, norm_gain.reshape(1, nt * width), attn_query, attn_key, attn_value, delta_query,
        delta_key, delta_value, delta_gate, attn_out.T, delta_out.T, gates(beta_weight),
        gates(decay_weight), beta_shift, decay_log, sink_logit, out_gain.reshape(1, hd),
    )])


def solution(mesh):
    return jax.shard_map(
        per_device,
        mesh=mesh,
        in_specs=(
            P("sp", "tp"), P(), P("sp", "tp"), P("sp", "tp"), P("sp", "tp"), P("tp"),
            P("sp", "tp"), P("sp", "tp"), P("sp", "tp"), P("sp", "tp"),
            P("sp", "tp", None), P("sp", "tp", None), P(None, "tp"), P(None, "tp"), P(),
            P("tp", "sp"), P("tp", "sp"),
        ),
        out_specs=P(("sp", "tp"), None),
        check_vma=False,
    )
```

```python
import functools

import jax
import jax.numpy as jnp
from jax import lax
from jax.experimental import pallas as pl
from jax.experimental.pallas import tpu as pltpu
from jax.sharding import PartitionSpec as P

HEAD_DIM = 64
WINDOW = 64
norm_eps = 1e-06
MESH = pl.DeviceIdType.MESH
F32 = jnp.float32
BF16 = jnp.bfloat16
RING = 4


def exact(a, b, dims=((1,), (0,))):
    return lax.dot_general(
        a, b, (dims, ((), ())), precision=lax.Precision.HIGHEST, preferred_element_type=F32
    )


def plain(a, b, dims=((1,), (0,))):
    return lax.dot_general(a, b, (dims, ((), ())), preferred_element_type=F32)


def split(x):
    high = x.astype(BF16)
    return high, (x - high.astype(F32)).astype(BF16)


def close(a, b, dims=((1,), (0,))):
    (ca,), (cb,) = dims
    left = jnp.concatenate([a[0], a[1], a[0]], axis=ca)
    right = jnp.concatenate([b[0], b[0], b[1]], axis=cb)
    return plain(left, right, dims)


def near(a, b, dims=((1,), (0,))):
    a, b = split(a), split(b)
    return plain(a[0], b[0], dims) + (plain(a[1], b[0], dims) + plain(a[0], b[1], dims))


def silu(x):
    return x * jax.nn.sigmoid(x)


def unit_rows(x):
    return x * lax.rsqrt(jnp.sum(x * x, axis=-1, keepdims=True) + norm_eps)


def copy_to(src, dst, send, recv, device):
    return pltpu.make_async_remote_copy(
        src_ref=src,
        dst_ref=dst,
        send_sem=send,
        recv_sem=recv,
        device_id=device,
        device_id_type=MESH,
    )


class Spread:
    def __init__(self, core, z, y, t, rows, own, send_sem, recv_sem, single=False):
        self.core, self.z, self.y, self.t = core, z, y, t
        self.rows, self.own, self.send_sem, self.recv_sem = rows, own, send_sem, recv_sem
        self.single, self.axes = single, (core,) if single else (0, 1)
        self.partner = 2 * (z * RING + y) + 1 - core
        self.started = []

    def chip(self, axis, da, db):
        dz, dy = db + axis * (da - db), da + axis * (db - da)
        return lax.rem(self.z + dz + RING, RING) * RING + lax.rem(self.y + dy + RING, RING)

    def send(self, src, blk, device):
        k = len(self.started)
        c = copy_to(src, self.rows(blk), self.send_sem.at[k], self.recv_sem.at[blk], (device, self.t))
        c.start()
        self.started.append(c)

    def landed(self, blk):
        ref = self.rows(blk)
        copy_to(ref, ref, self.send_sem.at[0], self.recv_sem.at[blk], (self.partner, self.t)).wait_recv()

    def begin(self):
        me = 2 * self.chip(0, 0, 0) + self.core
        for da in (2, 1, -1):
            for axis in (0, 1):
                to = 2 * self.chip(axis, da, 0)
                if self.single:
                    self.send(self.own(self.core), me, to + self.core)
                else:
                    for c in range(2):
                        self.send(self.own(c), me, to + c)
        if not self.single:
            self.send(self.own(1 - self.core), me, self.partner)

    def forward(self):
        for r in (1, -1, 2):
            for axis in self.axes:
                blk = 2 * self.chip(axis, r, 0) + axis
                self.landed(blk)
                for db in (2, 1, -1):
                    self.send(self.rows(blk), blk, 2 * self.chip(axis, 0, db) + self.core)

    def finish(self, dbs=(1, -1, 2)):
        for r in (0, 1, -1, 2):
            for axis in self.axes:
                for db in dbs:
                    self.landed(2 * self.chip(axis, r, db) + axis)
        if not self.single:
            self.landed(self.partner)

    def drain(self):
        for c in self.started:
            c.wait_send()


def layer_kernel(
    n, nt,
    tok_in, gain_in, aq_in, ak_in, av_in, dq_in, dk_in, dv_in, dz_in, ao_in, do_in, bw_in, gw_in,
    shift_in, dlog_in, sink_src, og_in, out,
    gain, wide_in, slim_in, oin, bw, gw, shift, dlog, sink_in, og, in_sem,
    tokbuf, normed, pack1, pack2, wbuf1, wbuf2, obuf, acc1, acc2, kvbuf, st, stbuf, o_loc, r_mat, heads, gath,
    tok_s, tok_r, w1_s, w1_r, w2_s, w2_r, x_s, x_r, g_s, g_r, o_s, o_r, kv_s, kv_r, st_s, st_r, h_s, h_r,
):
    me, t = lax.axis_index("sp"), lax.axis_index("tp")
    rows, width = tok_in.shape
    kb = aq_in.shape[0]
    hd = HEAD_DIM
    chips = n // 2
    core, chip = lax.rem(me, 2), lax.div(me, 2)
    z, y = lax.div(chip, RING), lax.rem(chip, RING)
    partner = me + 1 - 2 * core
    mine = pl.ds(me * kb, kb)

    loads = [
        (bw_in, bw), (gw_in, gw), (ak_in, slim_in.at[0]), (av_in, slim_in.at[1]),
        (aq_in, wide_in.at[0]), (dq_in, wide_in.at[1]), (dk_in, wide_in.at[2]),
        (dv_in, wide_in.at[3]), (dz_in, wide_in.at[4]), (ao_in, oin.at[0]), (do_in, oin.at[1]),
        (tok_in, tokbuf.at[t, core]), (gain_in, gain), (shift_in, shift), (dlog_in, dlog),
        (sink_src, sink_in), (og_in, og),
    ]
    loads = [pltpu.make_async_copy(a, b, in_sem.at[i]) for i, (a, b) in enumerate(loads)]
    for c in loads:
        c.start()

    rows_of = lambda buf: lambda blk: buf.at[pl.ds(blk * kb, kb)]
    o_rows = lambda blk: obuf.at[t, lax.div(blk, 2 * RING), lax.rem(lax.div(blk, 2), RING), lax.rem(blk, 2)]
    w1 = Spread(core, z, y, t, rows_of(wbuf1), lambda c: pack1.at[c], w1_s, w1_r)
    w2 = Spread(core, z, y, t, rows_of(wbuf2), lambda c: pack2.at[c], w2_s, w2_r)
    os = Spread(core, z, y, t, o_rows, lambda c: o_rows(me), o_s, o_r, single=True)
    bar = pltpu.get_barrier_semaphore()
    pl.semaphore_signal(bar, inc=1, device_id=(partner, t), device_id_type=MESH)
    for d in range(1, nt):
        pl.semaphore_signal(bar, inc=1, device_id=(me, lax.rem(t + d, nt)), device_id_type=MESH)
    for da in (2, 1, -1):
        for axis in (0, 1):
            for c in range(2):
                p = 2 * w1.chip(axis, da, 0) + c
                pl.semaphore_signal(bar, inc=1, device_id=(p, t), device_id_type=MESH)

    for c in loads:
        c.wait()
    gates = [bw[...], gw[...]]
    lines = []
    for c in range(2):
        lines += [g[2 * c : 2 * c + 2].astype(F32) for g in gates]
        lines.append(jnp.zeros((hd - 4, kb), F32))
    gates = jnp.concatenate(lines, axis=0)
    gates = jnp.concatenate([gates, jnp.zeros((2 * hd, 2 * hd - kb), F32)], axis=1)
    gates = gates.T[:kb].astype(BF16)
    packs = ([], [])
    for c in range(2):
        half = slice(c * hd, (c + 1) * hd)
        aq, dq, dk, dv, dz = [wide_in[i][:, half] for i in range(5)]
        packs[0].append(jnp.concatenate([dk, dv, dq, gates[:, half]], axis=1))
        packs[1].append(jnp.concatenate([aq, dz, slim_in[0], slim_in[1]], axis=1))
        pack1[c], pack2[c] = packs[0][c], packs[1][c]
    wbuf1[mine] = jnp.where(core == 0, packs[0][0], packs[0][1])
    wbuf2[mine] = jnp.where(core == 0, packs[1][0], packs[1][1])
    obuf[t, z, y, core] = jnp.concatenate(
        [oin[0][:, :hd], oin[1][:, :hd], oin[0][:, hd:], oin[1][:, hd:]], axis=1
    )
    pl.semaphore_wait(bar, 12 + nt)

    w1.begin()

    def tok_copy(k, j, c, device):
        ref = tokbuf.at[j, c]
        return copy_to(ref, ref, tok_s.at[k], tok_r.at[j, c], device)

    tok_copies = [
        tok_copy(d - 1, t, core, (me, lax.rem(t + d, nt))) for d in (1, 3, 2)
    ] + [tok_copy(nt - 1, t, core, (partner, t))]
    for c in tok_copies:
        c.start()

    os.begin()
    w2.begin()
    w1.forward()
    for d in range(1, nt):
        j = lax.rem(t + d, nt)
        tok_copy(0, j, core, (partner, t)).wait_recv()
        c = tok_copy(nt - 1 + d, j, core, (partner, t))
        c.start()
        tok_copies.append(c)

    def norm(c):
        place = pl.ds(pl.multiple_of(c * rows, rows), rows)
        total = jnp.zeros((rows, 1), F32)
        for j in range(nt):
            x = tokbuf[j, c].astype(F32)
            total += jnp.sum(x * x, axis=-1, keepdims=True)
        inverse = lax.rsqrt(total / (nt * width) + norm_eps)
        for j in range(nt):
            cols = slice(j * width, (j + 1) * width)
            normed[place, cols] = (tokbuf[j, c].astype(F32) * inverse * gain[:, cols]).astype(BF16)

    norm(core)
    for j in range(nt):
        tok_copy(0, j, 1 - core, (partner, t)).wait_recv()
    norm(1 - core)
    os.forward()

    def own_class(act):
        for c in range(2):
            pl.when(core == c)(lambda c=c: act(c))

    def band(db, c, j):
        if c == 0:
            return obuf.at[j, lax.rem(z + db, RING), :, 0]
        return obuf.at[j, :, lax.rem(y + db, RING), 1]

    def x_copy(db, d, c, j):
        ref = band(db, c, j)
        return copy_to(ref, ref, x_s.at[db, d - 1], x_r.at[db, j], (me, lax.rem(t + d, nt)))

    def x_all(db, act):
        for d in range(1, nt):
            own_class(lambda c, d=d: act(x_copy(db, d, c, t)))

    def share(db, c):
        ref = band(db, c, slice(None))
        return copy_to(ref, ref, g_s.at[db], g_r.at[db], (partner, t))

    def pass_on(db):
        for d in range(1, nt):
            own_class(lambda c, d=d: x_copy(db, d, c, lax.rem(t + d, nt)).wait_recv())
        own_class(lambda c: share(db, c).start())

    x_all(0, lambda c: c.start())
    w2.forward()
    w1.finish()

    acc1[...] = plain(normed[...], wbuf1[...])
    lane = lax.broadcasted_iota(jnp.int32, (1, 2 * hd), 1)
    shift_row = jnp.where(lane == hd, shift[0, core], shift[1, core])
    dlog_row = jnp.where(lane == hd + 2, dlog[0, core], dlog[1, core])
    coef = jnp.where((lane == hd + 2) | (lane == hd + 3), -jnp.exp(dlog_row) / (rows * n), 0.0)
    ri = lax.broadcasted_iota(jnp.int32, (rows, rows), 0)
    ci = lax.broadcasted_iota(jnp.int32, (rows, rows), 1)
    incl = (ri >= ci, ri <= ci)
    strict = (ri > ci, ri < ci)
    ones = [jnp.where(m, 1.0, 0.0).astype(F32) for m in incl]
    chains = []
    for j in range(2):
        part_rows = slice(j * rows, (j + 1) * rows)
        tail = acc1[part_rows, 2 * hd :]
        soft = jnp.maximum(tail, 0.0) + jnp.log1p(jnp.exp(-jnp.abs(tail)))
        g = coef * soft
        hi_g = g.astype(BF16)
        mid = (g - hi_g.astype(F32))
        mid_g = mid.astype(BF16)
        low_g = (mid - mid_g.astype(F32)).astype(BF16)
        gs = jnp.concatenate([hi_g, mid_g, low_g], axis=0)
        cums = [plain(jnp.concatenate([m.astype(BF16)] * 3, axis=1), gs) for m in ones]
        columns = jnp.where(
            lane == hd + 2, cums[0],
            jnp.where(lane == hd + 3, cums[1], jax.nn.sigmoid(tail + shift_row)),
        )
        lines = columns.T

        def cols(i):
            return acc1[part_rows, i * hd : (i + 1) * hd].astype(BF16).astype(F32)

        q = unit_rows(silu(cols(2))) * hd ** (-0.5)
        k = unit_rows(silu(cols(0)))
        v = silu(cols(1))
        kk = near(k, k, ((1,), (1,)))
        qk = near(q, k, ((1,), (1,)))
        for r in range(2):
            at = hd + 2 + r
            gcol = columns[:, at : at + 1]
            grow = lines[at : at + 1, :]
            beta = columns[:, hd + r : hd + r + 1]
            decay = jnp.where(incl[r], jnp.exp(jnp.minimum(gcol - grow, 0.0)), 0.0)
            a = jnp.where(strict[r], beta * kk * decay, 0.0)
            eg = jnp.exp(gcol)
            last = gcol[rows - 1 : rows, :] if r == 0 else gcol[0:1, :]
            chains.append(
                dict(
                    r=r, j=j, a=a, rhs=jnp.concatenate([beta * v, beta * k * eg], axis=1),
                    pm=qk * decay, qe=q * eg, kd=(k * jnp.exp(last - gcol)).T, last=last,
                )
            )
    levels = rows.bit_length() - 1
    eye = jnp.where(ri == ci, 1.0, 0.0).astype(F32)
    xor = ri ^ ci
    inv = [eye - jnp.where(xor == 1, ch["a"], 0.0) for ch in chains]
    pairs = [split(ch["a"]) for ch in chains]
    for lv in range(1, levels):
        m = jnp.where((xor >> lv) == 1, 1.0, 0.0).astype(BF16)
        xs = [split(x) for x in inv]
        left = [close(x, (m * a[0], m * a[1])) for x, a in zip(xs, pairs)]
        inv = [x - close(split(y_), z_) for x, y_, z_ in zip(inv, left, xs)]
    for db in (1, 3, 2):
        os.finish((db if db < 3 else -1,))
        x_all(db, lambda c: c.start())
    sols = [split(close(split(x), split(ch["rhs"]))) for x, ch in zip(inv, chains)]
    outs = [close(split(ch["kd"]), s) for ch, s in zip(chains, sols)]
    e64 = jnp.where(
        lax.broadcasted_iota(jnp.int32, (hd, hd), 0)
        == lax.broadcasted_iota(jnp.int32, (hd, hd), 1), 1.0, 0.0,
    ).astype(F32)
    moves = [
        jnp.concatenate([s[:, :hd], jnp.exp(ch["last"]) * e64 - s[:, hd:]], axis=1)
        for ch, s in zip(chains, outs)
    ]
    none = jnp.zeros((hd, hd), F32)
    for r in range(2):
        early, late = moves[2 * r + r], moves[2 * (1 - r) + r]
        full = close(split(late[:, hd:]), split(early))
        full += jnp.concatenate([late[:, :hd], none], axis=1)
        st[r] = full.astype(BF16)

    offsets = sorted(
        [(dz, dy) for dz in (0, 1, -1, 2) for dy in (0, 1, -1, 2) if dz or dy], key=lambda o: -abs(o[0]) - abs(o[1])
    )

    def state_copy(k):
        p = w1.chip(0, offsets[k][1], offsets[k][0])
        return copy_to(
            st.at[jnp.where(p > chip, 0, 1)], stbuf.at[chip], st_s.at[k], st_r.at[chip], (2 * p + core, t)
        )

    states = [state_copy(k) for k in range(chips - 1)]
    for c in states:
        c.start()
    w2.finish()
    acc2[...] = plain(normed[...], wbuf2[...])
    both = 2 * rows
    kvbuf[WINDOW : WINDOW + both] = acc2[:, 2 * hd :].astype(BF16)

    @pl.when(chip == 0)
    def _():
        kvbuf[:WINDOW] = jnp.zeros((WINDOW, 2 * hd), BF16)

    @pl.when(chip == chips - 1)
    def _():
        kvbuf[WINDOW + both :] = jnp.zeros((WINDOW, 2 * hd), BF16)

    def halo(p):
        up = copy_to(
            kvbuf.at[pl.ds(both, WINDOW)], kvbuf.at[pl.ds(0, WINDOW)],
            kv_s.at[0], kv_r.at[0], (me + 2, t),
        )
        down = copy_to(
            kvbuf.at[pl.ds(WINDOW, WINDOW)], kvbuf.at[pl.ds(WINDOW + both, WINDOW)],
            kv_s.at[1], kv_r.at[1], (me - 2, t),
        )
        return (up, down)[p]

    pl.when(chip < chips - 1)(lambda: halo(0).start())
    pl.when(chip > 0)(lambda: halo(1).start())
    inner = [close(split(ch["pm"]), s) for ch, s in zip(chains, sols)]
    for ch, s in zip(chains, inner):
        j, r = ch["j"], ch["r"]
        local, reach = s[:, :hd], ch["qe"] - s[:, hd:]
        if j != r:
            step = close(split(reach), split(moves[2 * (1 - j) + r]))
            local, reach = local + step[:, :hd], step[:, hd:]
        o_loc[j, r] = local
        r_mat[j, r] = reach

    pass_on(0)
    pl.when(chip > 0)(lambda: halo(0).wait_recv())
    pl.when(chip < chips - 1)(lambda: halo(1).wait_recv())
    span = rows + 2 * WINDOW
    qi = lax.broadcasted_iota(jnp.int32, (rows, span), 0)
    kj = lax.broadcasted_iota(jnp.int32, (rows, span), 1) - WINDOW
    sink = sink_in[core]
    for j in range(2):
        pos = kj + (2 * chip + j) * rows
        allowed = (jnp.abs(qi - kj) <= WINDOW) & (pos >= 0) & (pos < n * rows)
        q = acc2[j * rows : (j + 1) * rows, :hd].astype(BF16)
        keys = slice(j * rows, j * rows + span)
        s = plain(q, kvbuf[keys, :hd], ((1,), (1,))) * hd ** (-0.5)
        s = jnp.where(allowed, s, -jnp.inf)
        m = jnp.maximum(jnp.max(s, axis=-1, keepdims=True), sink)
        e = jnp.exp(s - m)
        p = e / (jnp.sum(e, axis=-1, keepdims=True) + jnp.exp(sink - m))
        heads[j, :, :hd] = plain(p.astype(BF16), kvbuf[keys, hd:]).astype(BF16)

    for d in range(1, chips):
        there = lax.rem(chip + d, chips)
        copy_to(st.at[0], stbuf.at[there], st_s.at[0], st_r.at[there], (me, t)).wait_recv()

    def follow(late, early):
        full = close(split(late[:, hd:]), split(early))
        return full + jnp.concatenate([late[:, :hd], none], axis=1)

    def first_follow(late, early):
        full = plain(late[:, hd:], early)
        return full + jnp.concatenate([late[:, :hd].astype(F32), none], axis=1)

    ident = jnp.concatenate([none, e64], axis=1)
    kin = []
    for level in range(4):
        size = 1 << level
        before = lax.rem(lax.div(chip, size), 2) == 1
        base = (lax.div(chip, size) + jnp.where(before, -1, 1)) * size
        group = [stbuf[base + i] for i in range(size)]
        merge = first_follow
        while len(group) > 1:
            group = [
                merge(jnp.where(before, hi, lo), jnp.where(before, lo, hi))
                for lo, hi in zip(group[::2], group[1::2])
            ]
            merge = follow
        kin.append((before, group[0].astype(F32)))
    sums = []
    for r in range(2):
        steps = [jnp.where(ok if r == 0 else ~ok, move, ident) for ok, move in kin]
        near_part = follow(follow(steps[0], steps[1]), steps[2])
        sums.append(near(near_part[:, hd:], steps[3][:, :hd]) + near_part[:, :hd])
    pass_on(1)
    for j in range(2):
        o = o_loc[j, 0] + o_loc[j, 1]
        reach = split(jnp.concatenate([r_mat[j, 0], r_mat[j, 1]], axis=1))
        o += close(reach, split(jnp.concatenate(sums, axis=0)))
        o = o * lax.rsqrt(jnp.mean(o * o, axis=-1, keepdims=True) + norm_eps) * og[...]
        gate = acc2[j * rows : (j + 1) * rows, hd : 2 * hd].astype(BF16).astype(F32)
        heads[j, :, hd:] = (o * silu(gate)).astype(BF16)

    tr = rows // nt
    spot = lambda x: pl.ds(pl.multiple_of(x * tr, tr), tr)
    peers = [(lax.rem(t + d, nt), c) for d in range(1, nt) for c in (core, 1 - core)]
    peers.append((t, 1 - core))

    def hand(k, x, c):
        return copy_to(
            heads.at[c, spot(x)], gath.at[2 * t + core], h_s.at[k], h_r.at[2 * t + core], (2 * chip + c, x)
        )

    hands = [hand(k, x, c) for k, (x, c) in enumerate(peers)]
    for c in hands:
        c.start()
    gath[2 * t + core] = heads[core, spot(t)]
    for c in tok_copies:
        c.wait_send()
    w1.drain()
    w2.drain()
    os.drain()
    for db in (3, 2):
        pass_on(db)
    for db in range(RING):
        x_all(db, lambda c: c.wait_send())
        own_class(lambda c: share(db, c).wait_send())
        own_class(lambda c: share(db, 1 - c).wait_recv())
    pl.when(chip < chips - 1)(lambda: halo(0).wait_send())
    pl.when(chip > 0)(lambda: halo(1).wait_send())
    for c in states:
        c.wait_send()
    for x, c in peers:
        ref = gath.at[2 * x + c]
        copy_to(ref, ref, h_s.at[0], h_r.at[2 * x + c], (2 * chip + c, x)).wait_recv()
    total = jnp.zeros(out.shape, F32)
    for x in range(nt):
        lhs = jnp.concatenate([gath[2 * x], gath[2 * x + 1]], axis=1)
        total += plain(lhs, obuf[x].reshape(n * kb, -1), ((1,), (1,)))
    out[...] = total.astype(BF16)
    for c in hands:
        c.wait_send()


def per_device(
    tokens, norm_gain, attn_query, attn_key, attn_value, sink_logit, delta_query, delta_key,
    delta_value, delta_gate, beta_weight, decay_weight, beta_shift, decay_log, out_gain,
    attn_out, delta_out,
):
    n, nt = lax.axis_size("sp"), lax.axis_size("tp")
    rows, width = tokens.shape
    kb = attn_query.shape[0]
    hd = HEAD_DIM
    cw = attn_out.shape[1]
    tr = rows // nt
    chips = n // 2
    assert n == 2 * RING * RING and cw == kb and rows == 2 * hd
    assert attn_query.shape[1] == delta_query.shape[1] == 2 * attn_key.shape[1] == 2 * hd
    gates = lambda w: jnp.transpose(w, (1, 2, 0)).reshape(4, kb)
    dma = pltpu.SemaphoreType.DMA
    vm, sm = pltpu.VMEM, pltpu.SMEM
    hbm = pl.BlockSpec(memory_space=pltpu.HBM)
    return pl.pallas_call(
        functools.partial(layer_kernel, n, nt),
        out_shape=jax.ShapeDtypeStruct((tr, n * cw), BF16),
        in_specs=[hbm] * 17,
        out_specs=pl.BlockSpec(memory_space=pltpu.VMEM),
        scratch_shapes=[
            vm((1, nt * width), F32),
            vm((5, kb, 2 * hd), BF16),
            vm((2, kb, hd), BF16),
            vm((2, cw, 2 * hd), BF16),
            vm((4, kb), BF16),
            vm((4, kb), BF16),
            sm((2, 2), F32),
            sm((2, 2), F32),
            sm((2,), F32),
            vm((1, hd), F32),
            dma((17,)),
            vm((nt, 2, rows, width), BF16),
            vm((2 * rows, nt * width), BF16),
            vm((2, kb, 4 * hd), BF16),
            vm((2, kb, 4 * hd), BF16),
            vm((n * kb, 4 * hd), BF16),
            vm((n * kb, 4 * hd), BF16),
            vm((nt, RING, RING, 2, cw, 4 * hd), BF16),
            vm((2 * rows, 4 * hd), F32),
            vm((2 * rows, 4 * hd), F32),
            vm((2 * rows + 2 * WINDOW, 2 * hd), BF16),
            vm((2, hd, 2 * hd), BF16),
            vm((chips, hd, 2 * hd), BF16),
            vm((2, 2, rows, hd), F32),
            vm((2, 2, rows, hd), F32),
            vm((2, rows, 2 * hd), BF16),
            vm((2 * nt, tr, 2 * hd), BF16),
            dma((2 * nt - 1,)), dma((nt, 2)),
            dma((n - 1,)), dma((n,)),
            dma((n - 1,)), dma((n,)),
            dma((RING, nt - 1)), dma((RING, nt)),
            dma((RING,)), dma((RING,)),
            dma((n - 1,)), dma((n,)),
            dma((2,)), dma((2,)),
            dma((chips,)), dma((chips,)),
            dma((2 * nt - 1,)), dma((2 * nt,)),
        ],
        compiler_params=pltpu.CompilerParams(
            collective_id=0, has_side_effects=True, vmem_limit_bytes=48*1024*1024
        ),
    )(*[pltpu.with_memory_space_constraint(x, pltpu.HBM) for x in (
        tokens, norm_gain.reshape(1, nt * width), attn_query, attn_key, attn_value, delta_query,
        delta_key, delta_value, delta_gate, attn_out.T, delta_out.T, gates(beta_weight),
        gates(decay_weight), beta_shift, decay_log, sink_logit, out_gain.reshape(1, hd),
    )])


def solution(mesh):
    return jax.shard_map(
        per_device,
        mesh=mesh,
        in_specs=(
            P("sp", "tp"), P(), P("sp", "tp"), P("sp", "tp"), P("sp", "tp"), P("tp"),
            P("sp", "tp"), P("sp", "tp"), P("sp", "tp"), P("sp", "tp"),
            P("sp", "tp", None), P("sp", "tp", None), P(None, "tp"), P(None, "tp"), P(),
            P("tp", "sp"), P("tp", "sp"),
        ),
        out_specs=P(("sp", "tp"), None),
        check_vma=False,
    )
```

```python
import functools

import jax
import jax.numpy as jnp
from jax import lax
from jax.experimental import pallas as pl
from jax.experimental.pallas import tpu as pltpu
from jax.sharding import PartitionSpec as P

HEAD_DIM = 64
WINDOW = 64
norm_eps = 1e-06
MESH = pl.DeviceIdType.MESH
F32 = jnp.float32
BF16 = jnp.bfloat16
RING = 4


def exact(a, b, dims=((1,), (0,))):
    return lax.dot_general(
        a, b, (dims, ((), ())), precision=lax.Precision.HIGHEST, preferred_element_type=F32
    )


def plain(a, b, dims=((1,), (0,))):
    return lax.dot_general(a, b, (dims, ((), ())), preferred_element_type=F32)


def split(x):
    high = x.astype(BF16)
    return high, (x - high.astype(F32)).astype(BF16)


def close(a, b, dims=((1,), (0,))):
    (ca,), (cb,) = dims
    left = jnp.concatenate([a[0], a[1], a[0]], axis=ca)
    right = jnp.concatenate([b[0], b[0], b[1]], axis=cb)
    return plain(left, right, dims)


def near(a, b, dims=((1,), (0,))):
    a, b = split(a), split(b)
    return plain(a[0], b[0], dims) + (plain(a[1], b[0], dims) + plain(a[0], b[1], dims))


def silu(x):
    return x * jax.nn.sigmoid(x)


def unit_rows(x):
    return x * lax.rsqrt(jnp.sum(x * x, axis=-1, keepdims=True) + norm_eps)


def copy_to(src, dst, send, recv, device):
    return pltpu.make_async_remote_copy(
        src_ref=src,
        dst_ref=dst,
        send_sem=send,
        recv_sem=recv,
        device_id=device,
        device_id_type=MESH,
    )


class Spread:
    def __init__(self, core, z, y, t, rows, own, send_sem, recv_sem, single=False):
        self.core, self.z, self.y, self.t = core, z, y, t
        self.rows, self.own, self.send_sem, self.recv_sem = rows, own, send_sem, recv_sem
        self.single, self.axes = single, (core,) if single else (0, 1)
        self.partner = 2 * (z * RING + y) + 1 - core
        self.started = []

    def chip(self, axis, da, db):
        dz, dy = db + axis * (da - db), da + axis * (db - da)
        return lax.rem(self.z + dz + RING, RING) * RING + lax.rem(self.y + dy + RING, RING)

    def send(self, src, blk, device):
        k = len(self.started)
        c = copy_to(src, self.rows(blk), self.send_sem.at[k], self.recv_sem.at[blk], (device, self.t))
        c.start()
        self.started.append(c)

    def landed(self, blk):
        ref = self.rows(blk)
        copy_to(ref, ref, self.send_sem.at[0], self.recv_sem.at[blk], (self.partner, self.t)).wait_recv()

    def begin(self):
        me = 2 * self.chip(0, 0, 0) + self.core
        for da in (2, 1, -1):
            for axis in (0, 1):
                to = 2 * self.chip(axis, da, 0)
                if self.single:
                    self.send(self.own(self.core), me, to + self.core)
                else:
                    for c in range(2):
                        self.send(self.own(c), me, to + c)
        if not self.single:
            self.send(self.own(1 - self.core), me, self.partner)

    def forward(self):
        for r in (1, -1, 2):
            for axis in self.axes:
                blk = 2 * self.chip(axis, r, 0) + axis
                self.landed(blk)
                for db in (2, 1, -1):
                    self.send(self.rows(blk), blk, 2 * self.chip(axis, 0, db) + self.core)

    def finish(self, dbs=(1, -1, 2)):
        for r in (0, 1, -1, 2):
            for axis in self.axes:
                for db in dbs:
                    self.landed(2 * self.chip(axis, r, db) + axis)
        if not self.single:
            self.landed(self.partner)

    def drain(self):
        for c in self.started:
            c.wait_send()


def layer_kernel(
    n, nt,
    tok_in, gain_in, aq_in, ak_in, av_in, dq_in, dk_in, dv_in, dz_in, ao_in, do_in, bw_in, gw_in,
    shift_in, dlog_in, sink_src, og_in, out,
    gain, wide_in, slim_in, oin, bw, gw, shift, dlog, sink_in, og, in_sem,
    tokbuf, normed, pack1, pack2, wbuf1, wbuf2, obuf, acc1, acc2, kvbuf, st, stbuf, o_loc, r_mat, heads, gath,
    tok_s, tok_r, w1_s, w1_r, w2_s, w2_r, x_s, x_r, g_s, g_r, o_s, o_r, kv_s, kv_r, st_s, st_r, h_s, h_r,
):
    me, t = lax.axis_index("sp"), lax.axis_index("tp")
    rows, width = tok_in.shape
    kb = aq_in.shape[0]
    hd = HEAD_DIM
    chips = n // 2
    core, chip = lax.rem(me, 2), lax.div(me, 2)
    z, y = lax.div(chip, RING), lax.rem(chip, RING)
    partner = me + 1 - 2 * core
    mine = pl.ds(me * kb, kb)

    loads = [
        (bw_in, bw), (gw_in, gw), (ak_in, slim_in.at[0]), (av_in, slim_in.at[1]),
        (aq_in, wide_in.at[0]), (dq_in, wide_in.at[1]), (dk_in, wide_in.at[2]),
        (dv_in, wide_in.at[3]), (dz_in, wide_in.at[4]), (ao_in, oin.at[0]), (do_in, oin.at[1]),
        (tok_in, tokbuf.at[t, core]), (gain_in, gain), (shift_in, shift), (dlog_in, dlog),
        (sink_src, sink_in), (og_in, og),
    ]
    loads = [pltpu.make_async_copy(a, b, in_sem.at[i]) for i, (a, b) in enumerate(loads)]
    for c in loads:
        c.start()

    rows_of = lambda buf: lambda blk: buf.at[pl.ds(blk * kb, kb)]
    o_rows = lambda blk: obuf.at[t, lax.div(blk, 2 * RING), lax.rem(lax.div(blk, 2), RING), lax.rem(blk, 2)]
    w1 = Spread(core, z, y, t, rows_of(wbuf1), lambda c: pack1.at[c], w1_s, w1_r)
    w2 = Spread(core, z, y, t, rows_of(wbuf2), lambda c: pack2.at[c], w2_s, w2_r)
    os = Spread(core, z, y, t, o_rows, lambda c: o_rows(me), o_s, o_r, single=True)
    bar = pltpu.get_barrier_semaphore()
    pl.semaphore_signal(bar, inc=1, device_id=(partner, t), device_id_type=MESH)
    for d in range(1, nt):
        pl.semaphore_signal(bar, inc=1, device_id=(me, lax.rem(t + d, nt)), device_id_type=MESH)
    for da in (2, 1, -1):
        for axis in (0, 1):
            for c in range(2):
                p = 2 * w1.chip(axis, da, 0) + c
                pl.semaphore_signal(bar, inc=1, device_id=(p, t), device_id_type=MESH)

    for c in loads:
        c.wait()
    gates = [bw[...], gw[...]]
    lines = []
    for c in range(2):
        lines += [g[2 * c : 2 * c + 2].astype(F32) for g in gates]
        lines.append(jnp.zeros((hd - 4, kb), F32))
    gates = jnp.concatenate(lines, axis=0)
    gates = jnp.concatenate([gates, jnp.zeros((2 * hd, 2 * hd - kb), F32)], axis=1)
    gates = gates.T[:kb].astype(BF16)
    packs = ([], [])
    for c in range(2):
        half = slice(c * hd, (c + 1) * hd)
        aq, dq, dk, dv, dz = [wide_in[i][:, half] for i in range(5)]
        packs[0].append(jnp.concatenate([dk, dv, dq, gates[:, half]], axis=1))
        packs[1].append(jnp.concatenate([aq, dz, slim_in[0], slim_in[1]], axis=1))
        pack1[c], pack2[c] = packs[0][c], packs[1][c]
    wbuf1[mine] = jnp.where(core == 0, packs[0][0], packs[0][1])
    wbuf2[mine] = jnp.where(core == 0, packs[1][0], packs[1][1])
    obuf[t, z, y, core] = jnp.concatenate(
        [oin[0][:, :hd], oin[1][:, :hd], oin[0][:, hd:], oin[1][:, hd:]], axis=1
    )
    pl.semaphore_wait(bar, 12 + nt)

    w1.begin()

    def tok_copy(k, j, c, device):
        ref = tokbuf.at[j, c]
        return copy_to(ref, ref, tok_s.at[k], tok_r.at[j, c], device)

    tok_copies = [
        tok_copy(d - 1, t, core, (me, lax.rem(t + d, nt))) for d in (1, 3, 2)
    ] + [tok_copy(nt - 1, t, core, (partner, t))]
    for c in tok_copies:
        c.start()

    os.begin()
    w2.begin()
    w1.forward()
    for d in range(1, nt):
        j = lax.rem(t + d, nt)
        tok_copy(0, j, core, (partner, t)).wait_recv()
        c = tok_copy(nt - 1 + d, j, core, (partner, t))
        c.start()
        tok_copies.append(c)

    def norm(c):
        place = pl.ds(pl.multiple_of(c * rows, rows), rows)
        total = jnp.zeros((rows, 1), F32)
        for j in range(nt):
            x = tokbuf[j, c].astype(F32)
            total += jnp.sum(x * x, axis=-1, keepdims=True)
        inverse = lax.rsqrt(total / (nt * width) + norm_eps)
        for j in range(nt):
            cols = slice(j * width, (j + 1) * width)
            normed[place, cols] = (tokbuf[j, c].astype(F32) * inverse * gain[:, cols]).astype(BF16)

    norm(core)
    for j in range(nt):
        tok_copy(0, j, 1 - core, (partner, t)).wait_recv()
    norm(1 - core)
    os.forward()

    def own_class(act):
        for c in range(2):
            pl.when(core == c)(lambda c=c: act(c))

    def band(db, c, j):
        if c == 0:
            return obuf.at[j, lax.rem(z + db, RING), :, 0]
        return obuf.at[j, :, lax.rem(y + db, RING), 1]

    def x_copy(db, d, c, j):
        ref = band(db, c, j)
        return copy_to(ref, ref, x_s.at[db, d - 1], x_r.at[db, j], (me, lax.rem(t + d, nt)))

    def x_all(db, act):
        for d in range(1, nt):
            own_class(lambda c, d=d: act(x_copy(db, d, c, t)))

    def share(db, c):
        ref = band(db, c, slice(None))
        return copy_to(ref, ref, g_s.at[db], g_r.at[db], (partner, t))

    def pass_on(db):
        for d in range(1, nt):
            own_class(lambda c, d=d: x_copy(db, d, c, lax.rem(t + d, nt)).wait_recv())
        own_class(lambda c: share(db, c).start())

    x_all(0, lambda c: c.start())
    w2.forward()
    w1.finish()

    acc1[...] = plain(normed[...], wbuf1[...])
    lane = lax.broadcasted_iota(jnp.int32, (1, 2 * hd), 1)
    shift_row = jnp.where(lane == hd, shift[0, core], shift[1, core])
    dlog_row = jnp.where(lane == hd + 2, dlog[0, core], dlog[1, core])
    coef = jnp.where((lane == hd + 2) | (lane == hd + 3), -jnp.exp(dlog_row) / (rows * n), 0.0)
    ri = lax.broadcasted_iota(jnp.int32, (rows, rows), 0)
    ci = lax.broadcasted_iota(jnp.int32, (rows, rows), 1)
    incl = (ri >= ci, ri <= ci)
    strict = (ri > ci, ri < ci)
    ones = [jnp.where(m, 1.0, 0.0).astype(F32) for m in incl]
    chains = []
    for j in range(2):
        part_rows = slice(j * rows, (j + 1) * rows)
        tail = acc1[part_rows, 2 * hd :]
        soft = jnp.maximum(tail, 0.0) + jnp.log1p(jnp.exp(-jnp.abs(tail)))
        g = coef * soft
        hi_g = g.astype(BF16)
        mid = (g - hi_g.astype(F32))
        mid_g = mid.astype(BF16)
        low_g = (mid - mid_g.astype(F32)).astype(BF16)
        gs = jnp.concatenate([hi_g, mid_g, low_g], axis=0)
        cums = [plain(jnp.concatenate([m.astype(BF16)] * 3, axis=1), gs) for m in ones]
        columns = jnp.where(
            lane == hd + 2, cums[0],
            jnp.where(lane == hd + 3, cums[1], jax.nn.sigmoid(tail + shift_row)),
        )
        lines = columns.T

        def cols(i):
            return acc1[part_rows, i * hd : (i + 1) * hd].astype(BF16).astype(F32)

        q = unit_rows(silu(cols(2))) * hd ** (-0.5)
        k = unit_rows(silu(cols(0)))
        v = silu(cols(1))
        kk = near(k, k, ((1,), (1,)))
        qk = near(q, k, ((1,), (1,)))
        for r in range(2):
            at = hd + 2 + r
            gcol = columns[:, at : at + 1]
            grow = lines[at : at + 1, :]
            beta = columns[:, hd + r : hd + r + 1]
            decay = jnp.where(incl[r], jnp.exp(jnp.minimum(gcol - grow, 0.0)), 0.0)
            a = jnp.where(strict[r], beta * kk * decay, 0.0)
            eg = jnp.exp(gcol)
            last = gcol[rows - 1 : rows, :] if r == 0 else gcol[0:1, :]
            chains.append(
                dict(
                    r=r, j=j, a=a, rhs=jnp.concatenate([beta * v, beta * k * eg], axis=1),
                    pm=qk * decay, qe=q * eg, kd=(k * jnp.exp(last - gcol)).T, last=last,
                )
            )
    levels = rows.bit_length() - 1
    eye = jnp.where(ri == ci, 1.0, 0.0).astype(F32)
    xor = ri ^ ci
    inv = [eye - jnp.where(xor == 1, ch["a"], 0.0) for ch in chains]
    pairs = [split(ch["a"]) for ch in chains]
    for lv in range(1, levels):
        m = jnp.where((xor >> lv) == 1, 1.0, 0.0).astype(BF16)
        xs = [split(x) for x in inv]
        left = [close(x, (m * a[0], m * a[1])) for x, a in zip(xs, pairs)]
        inv = [x - close(split(y_), z_) for x, y_, z_ in zip(inv, left, xs)]
    for db in (1, 3, 2):
        os.finish((db if db < 3 else -1,))
        x_all(db, lambda c: c.start())
    sols = [split(close(split(x), split(ch["rhs"]))) for x, ch in zip(inv, chains)]
    outs = [close(split(ch["kd"]), s) for ch, s in zip(chains, sols)]
    e64 = jnp.where(
        lax.broadcasted_iota(jnp.int32, (hd, hd), 0)
        == lax.broadcasted_iota(jnp.int32, (hd, hd), 1), 1.0, 0.0,
    ).astype(F32)
    moves = [
        jnp.concatenate([s[:, :hd], jnp.exp(ch["last"]) * e64 - s[:, hd:]], axis=1)
        for ch, s in zip(chains, outs)
    ]
    none = jnp.zeros((hd, hd), F32)
    for r in range(2):
        early, late = moves[2 * r + r], moves[2 * (1 - r) + r]
        full = close(split(late[:, hd:]), split(early))
        full += jnp.concatenate([late[:, :hd], none], axis=1)
        st[r] = full.astype(BF16)

    offsets = sorted(
        [(dz, dy) for dz in (0, 1, -1, 2) for dy in (0, 1, -1, 2) if dz or dy], key=lambda o: -abs(o[0]) - abs(o[1])
    )

    def state_copy(k):
        p = w1.chip(0, offsets[k][1], offsets[k][0])
        return copy_to(
            st.at[jnp.where(p > chip, 0, 1)], stbuf.at[chip], st_s.at[k], st_r.at[chip], (2 * p + core, t)
        )

    states = [state_copy(k) for k in range(chips - 1)]
    for c in states:
        c.start()
    w2.finish()
    acc2[...] = plain(normed[...], wbuf2[...])
    both = 2 * rows
    kvbuf[WINDOW : WINDOW + both] = acc2[:, 2 * hd :].astype(BF16)

    @pl.when(chip == 0)
    def _():
        kvbuf[:WINDOW] = jnp.zeros((WINDOW, 2 * hd), BF16)

    @pl.when(chip == chips - 1)
    def _():
        kvbuf[WINDOW + both :] = jnp.zeros((WINDOW, 2 * hd), BF16)

    def halo(p):
        up = copy_to(
            kvbuf.at[pl.ds(both, WINDOW)], kvbuf.at[pl.ds(0, WINDOW)],
            kv_s.at[0], kv_r.at[0], (me + 2, t),
        )
        down = copy_to(
            kvbuf.at[pl.ds(WINDOW, WINDOW)], kvbuf.at[pl.ds(WINDOW + both, WINDOW)],
            kv_s.at[1], kv_r.at[1], (me - 2, t),
        )
        return (up, down)[p]

    pl.when(chip < chips - 1)(lambda: halo(0).start())
    pl.when(chip > 0)(lambda: halo(1).start())
    inner = [close(split(ch["pm"]), s) for ch, s in zip(chains, sols)]
    for ch, s in zip(chains, inner):
        j, r = ch["j"], ch["r"]
        local, reach = s[:, :hd], ch["qe"] - s[:, hd:]
        if j != r:
            step = close(split(reach), split(moves[2 * (1 - j) + r]))
            local, reach = local + step[:, :hd], step[:, hd:]
        o_loc[j, r] = local
        r_mat[j, r] = reach

    pass_on(0)
    pl.when(chip > 0)(lambda: halo(0).wait_recv())
    pl.when(chip < chips - 1)(lambda: halo(1).wait_recv())
    span = rows + 2 * WINDOW
    qi = lax.broadcasted_iota(jnp.int32, (rows, span), 0)
    kj = lax.broadcasted_iota(jnp.int32, (rows, span), 1) - WINDOW
    sink = sink_in[core]
    for j in range(2):
        pos = kj + (2 * chip + j) * rows
        allowed = (jnp.abs(qi - kj) <= WINDOW) & (pos >= 0) & (pos < n * rows)
        q = acc2[j * rows : (j + 1) * rows, :hd].astype(BF16)
        keys = slice(j * rows, j * rows + span)
        s = plain(q, kvbuf[keys, :hd], ((1,), (1,))) * hd ** (-0.5)
        s = jnp.where(allowed, s, -jnp.inf)
        m = jnp.maximum(jnp.max(s, axis=-1, keepdims=True), sink)
        e = jnp.exp(s - m)
        p = e / (jnp.sum(e, axis=-1, keepdims=True) + jnp.exp(sink - m))
        heads[j, :, :hd] = plain(p.astype(BF16), kvbuf[keys, hd:]).astype(BF16)

    for d in range(1, chips):
        there = lax.rem(chip + d, chips)
        copy_to(st.at[0], stbuf.at[there], st_s.at[0], st_r.at[there], (me, t)).wait_recv()

    def follow(late, early):
        full = close(split(late[:, hd:]), split(early))
        return full + jnp.concatenate([late[:, :hd], none], axis=1)

    def first_follow(late, early):
        full = plain(late[:, hd:], early)
        return full + jnp.concatenate([late[:, :hd].astype(F32), none], axis=1)

    ident = jnp.concatenate([none, e64], axis=1)
    kin = []
    for level in range(4):
        size = 1 << level
        before = lax.rem(lax.div(chip, size), 2) == 1
        base = (lax.div(chip, size) + jnp.where(before, -1, 1)) * size
        group = [stbuf[base + i] for i in range(size)]
        merge = first_follow
        while len(group) > 1:
            group = [
                merge(jnp.where(before, hi, lo), jnp.where(before, lo, hi))
                for lo, hi in zip(group[::2], group[1::2])
            ]
            merge = follow
        kin.append((before, group[0].astype(F32)))
    sums = []
    for r in range(2):
        steps = [jnp.where(ok if r == 0 else ~ok, move, ident) for ok, move in kin]
        near_part = follow(follow(steps[0], steps[1]), steps[2])
        sums.append(near(near_part[:, hd:], steps[3][:, :hd]) + near_part[:, :hd])
    pass_on(1)
    for j in range(2):
        o = o_loc[j, 0] + o_loc[j, 1]
        reach = split(jnp.concatenate([r_mat[j, 0], r_mat[j, 1]], axis=1))
        o += close(reach, split(jnp.concatenate(sums, axis=0)))
        o = o * lax.rsqrt(jnp.mean(o * o, axis=-1, keepdims=True) + norm_eps) * og[...]
        gate = acc2[j * rows : (j + 1) * rows, hd : 2 * hd].astype(BF16).astype(F32)
        heads[j, :, hd:] = (o * silu(gate)).astype(BF16)

    tr = rows // nt
    spot = lambda x: pl.ds(pl.multiple_of(x * tr, tr), tr)
    peers = [(lax.rem(t + d, nt), c) for d in range(1, nt) for c in (core, 1 - core)]
    peers.append((t, 1 - core))

    def hand(k, x, c):
        return copy_to(
            heads.at[c, spot(x)], gath.at[2 * t + core], h_s.at[k], h_r.at[2 * t + core], (2 * chip + c, x)
        )

    hands = [hand(k, x, c) for k, (x, c) in enumerate(peers)]
    for c in hands:
        c.start()
    gath[2 * t + core] = heads[core, spot(t)]
    for db in (3, 2):
        pass_on(db)
    for c in tok_copies:
        c.wait_send()
    w1.drain()
    w2.drain()
    os.drain()
    for db in range(RING):
        x_all(db, lambda c: c.wait_send())
        own_class(lambda c: share(db, c).wait_send())
        own_class(lambda c: share(db, 1 - c).wait_recv())
    pl.when(chip < chips - 1)(lambda: halo(0).wait_send())
    pl.when(chip > 0)(lambda: halo(1).wait_send())
    for c in states:
        c.wait_send()
    for x, c in peers:
        ref = gath.at[2 * x + c]
        copy_to(ref, ref, h_s.at[0], h_r.at[2 * x + c], (2 * chip + c, x)).wait_recv()
    total = jnp.zeros(out.shape, F32)
    for x in range(nt):
        lhs = jnp.concatenate([gath[2 * x], gath[2 * x + 1]], axis=1)
        total += plain(lhs, obuf[x].reshape(n * kb, -1), ((1,), (1,)))
    out[...] = total.astype(BF16)
    for c in hands:
        c.wait_send()


def per_device(
    tokens, norm_gain, attn_query, attn_key, attn_value, sink_logit, delta_query, delta_key,
    delta_value, delta_gate, beta_weight, decay_weight, beta_shift, decay_log, out_gain,
    attn_out, delta_out,
):
    n, nt = lax.axis_size("sp"), lax.axis_size("tp")
    rows, width = tokens.shape
    kb = attn_query.shape[0]
    hd = HEAD_DIM
    cw = attn_out.shape[1]
    tr = rows // nt
    chips = n // 2
    assert n == 2 * RING * RING and cw == kb and rows == 2 * hd
    assert attn_query.shape[1] == delta_query.shape[1] == 2 * attn_key.shape[1] == 2 * hd
    gates = lambda w: jnp.transpose(w, (1, 2, 0)).reshape(4, kb)
    dma = pltpu.SemaphoreType.DMA
    vm, sm = pltpu.VMEM, pltpu.SMEM
    hbm = pl.BlockSpec(memory_space=pltpu.HBM)
    return pl.pallas_call(
        functools.partial(layer_kernel, n, nt),
        out_shape=jax.ShapeDtypeStruct((tr, n * cw), BF16),
        in_specs=[hbm] * 17,
        out_specs=pl.BlockSpec(memory_space=pltpu.VMEM),
        scratch_shapes=[
            vm((1, nt * width), F32),
            vm((5, kb, 2 * hd), BF16),
            vm((2, kb, hd), BF16),
            vm((2, cw, 2 * hd), BF16),
            vm((4, kb), BF16),
            vm((4, kb), BF16),
            sm((2, 2), F32),
            sm((2, 2), F32),
            sm((2,), F32),
            vm((1, hd), F32),
            dma((17,)),
            vm((nt, 2, rows, width), BF16),
            vm((2 * rows, nt * width), BF16),
            vm((2, kb, 4 * hd), BF16),
            vm((2, kb, 4 * hd), BF16),
            vm((n * kb, 4 * hd), BF16),
            vm((n * kb, 4 * hd), BF16),
            vm((nt, RING, RING, 2, cw, 4 * hd), BF16),
            vm((2 * rows, 4 * hd), F32),
            vm((2 * rows, 4 * hd), F32),
            vm((2 * rows + 2 * WINDOW, 2 * hd), BF16),
            vm((2, hd, 2 * hd), BF16),
            vm((chips, hd, 2 * hd), BF16),
            vm((2, 2, rows, hd), F32),
            vm((2, 2, rows, hd), F32),
            vm((2, rows, 2 * hd), BF16),
            vm((2 * nt, tr, 2 * hd), BF16),
            dma((2 * nt - 1,)), dma((nt, 2)),
            dma((n - 1,)), dma((n,)),
            dma((n - 1,)), dma((n,)),
            dma((RING, nt - 1)), dma((RING, nt)),
            dma((RING,)), dma((RING,)),
            dma((n - 1,)), dma((n,)),
            dma((2,)), dma((2,)),
            dma((chips,)), dma((chips,)),
            dma((2 * nt - 1,)), dma((2 * nt,)),
        ],
        compiler_params=pltpu.CompilerParams(
            collective_id=0, has_side_effects=True, vmem_limit_bytes=48*1024*1024
        ),
    )(*[pltpu.with_memory_space_constraint(x, pltpu.HBM) for x in (
        tokens, norm_gain.reshape(1, nt * width), attn_query, attn_key, attn_value, delta_query,
        delta_key, delta_value, delta_gate, attn_out.T, delta_out.T, gates(beta_weight),
        gates(decay_weight), beta_shift, decay_log, sink_logit, out_gain.reshape(1, hd),
    )])


def solution(mesh):
    return jax.shard_map(
        per_device,
        mesh=mesh,
        in_specs=(
            P("sp", "tp"), P(), P("sp", "tp"), P("sp", "tp"), P("sp", "tp"), P("tp"),
            P("sp", "tp"), P("sp", "tp"), P("sp", "tp"), P("sp", "tp"),
            P("sp", "tp", None), P("sp", "tp", None), P(None, "tp"), P(None, "tp"), P(),
            P("tp", "sp"), P("tp", "sp"),
        ),
        out_specs=P(("sp", "tp"), None),
        check_vma=False,
    )
```
